32 devices in a mesh: sp: 8 (over z, x), tp: 4 (over y, core).
Axes of the slice: x: 2, y: 2, z: 4, core: 2. Of those that a mesh axis runs over, the one named last changes fastest.
Arguments:
- tokens: bfloat16 [4096, 4096], P('sp', 'tp'), may hold values from -8 to 8
- w_key: bfloat16 [4096, 2048], P(None, 'tp'), may hold values from -0.09375 to 0.09375
- w_value: bfloat16 [4096, 2048], P(None, 'tp'), may hold values from -0.09375 to 0.09375
- w_beta: bfloat16 [4096, 16], replicated, may hold values from -0.09375 to 0.09375
- w_decay: bfloat16 [4096, 16], replicated, may hold values from -0.09375 to 0.09375
- beta_bias: float32 [16], replicated, may hold values from -6 to -4
- decay_rate: float32 [16], replicated, as said below
- forgetting_increment: float32 [16, 4096], P('tp', 'sp')
- new_query: bfloat16 [16, 128], P('tp', 'sp'), may hold values from -6 to 6
- read_gain: bfloat16 [128], replicated, may hold values from 0.099609375 to 1.8984375
Outputs:
- state_cache: bfloat16 [16, 128, 128], P('tp', 'sp')
- first_read: float32 [16, 128], P('tp')
The draws below stay inside these ranges and needn't reach their ends.
Inputs may be any that keep to these rules, and one draw needn't show every extreme that they name: `decay_rate`: positive.
All inputs are finite; a program needn't handle non-finite values.
Results may differ from the reference program's by a relative error of at most 0.0075.
Values may be sent and summed in bfloat16 or wider, within the bound.
A program may use at most 64 MiB of HBM per device.

```python
import math
import jax
import jax.numpy as jnp
from jax import lax

D = 4096
HEADS = 16
DK = 128
DV = 128
BLOCK = 64
LENGTH = 4096


def draw_tokens(key, part):
    perturbation_seed, common_key = jax.random.split(key, 2)
    blocks = LENGTH // BLOCK
    noise = jnp.clip(jax.random.normal(perturbation_seed, (LENGTH, D), jnp.float32), -4.5, 4.5)
    common = jnp.clip(jax.random.normal(common_key, (blocks, D), jnp.float32), -4.5, 4.5)
    mixed = noise + 0.7 * jnp.repeat(common, BLOCK, axis=0)
    return mixed.astype(jnp.bfloat16)


def draw_decay_rate(key, part):
    slow_key, fast_key, pick_key = jax.random.split(key, 3)
    slow = jnp.exp(jax.random.uniform(slow_key, (HEADS,), jnp.float32, math.log(0.2 / LENGTH), math.log(1.0 / LENGTH)))
    fast = jnp.exp(jax.random.uniform(fast_key, (HEADS,), jnp.float32, math.log(0.02), math.log(0.06)))
    picked = jax.random.bernoulli(pick_key, 0.5, (HEADS,))
    return jnp.where(picked, fast, slow)


def draw_forgetting_increment(key, part):
    scale_key, location_seed, drop_key = jax.random.split(key, 3)
    blocks = LENGTH // BLOCK
    factor = jnp.exp(jax.random.uniform(scale_key, (HEADS, blocks), jnp.float32, math.log(0.25), math.log(4.0)))
    starting_displacement = -jnp.repeat(factor, BLOCK, axis=1) / LENGTH
    location_positions = jax.random.randint(location_seed, (HEADS, 4), 0, LENGTH)
    discarded_elements = jnp.log(jax.random.uniform(drop_key, (HEADS, 4), jnp.float32, 0.5, 0.8))
    breadth_across = jnp.arange(LENGTH)
    cluster_batches = jnp.sum(jnp.where(breadth_across[None, None, :] == location_positions[:, :, None], discarded_elements[:, :, None], 0.0), axis=1)
    return starting_displacement + cluster_batches


def levels(stream_key, dims, shards, least, largest):
    level, own = 1.0, jax.random.fold_in(stream_key, 6)
    for dim, shards_of in shards:
        draws = jnp.exp(jax.random.uniform(jax.random.fold_in(own, dim), (shards_of,), jnp.float32, least / len(shards), largest / len(shards)))
        level = level * jnp.repeat(draws, dims[dim] // shards_of).reshape([-1 if axis == dim else 1 for axis in range(len(dims))])
    return level


def centred(own_key, shape, scale, limit, pieces=(), kind=jnp.bfloat16):
    array = jax.random.normal(own_key, shape, jnp.float32) * scale
    if len(pieces) > 0:
        array = levels(own_key, shape, pieces, -0.22, 0.18) * array
    return jnp.clip(array, min=-limit, max=limit).astype(kind)


def setup_inputs(seed: int = 0) -> dict:
    streams_of = jax.random.split(jax.random.key(seed), 11)
    return {
        "tokens": draw_tokens(jax.random.fold_in(streams_of[10], 71), 0),
        "w_key": centred(streams_of[1], (D, HEADS * DK), D ** -0.5, 0.09375, ((1, 4),)),
        "w_value": centred(streams_of[2], (D, HEADS * DV), D ** -0.5, 0.09375, ((1, 4),)),
        "w_beta": centred(streams_of[3], (D, HEADS), D ** -0.5, 0.09375),
        "w_decay": centred(streams_of[4], (D, HEADS), D ** -0.5, 0.09375),
        "beta_bias": jnp.clip(jax.random.uniform(streams_of[5], (HEADS,), jnp.float32, -6.0, -4.0), -6.0, -4.0),
        "decay_rate": draw_decay_rate(jax.random.fold_in(streams_of[10], 71), 0),
        "forgetting_increment": draw_forgetting_increment(jax.random.fold_in(streams_of[10], 71), 0),
        "new_query": centred(streams_of[8], (HEADS, DK), 1.0, 6.0, ((0, 4), (1, 8))),
        "read_gain": jnp.clip(1.0 + 0.18 * jax.random.normal(streams_of[9], (DV,), jnp.float32), 0.099609375, 1.8984375).astype(jnp.bfloat16),
    }


norm_eps = 1e-06

def matmul_f32(left, right):
    return jnp.dot(left, right, precision=lax.Precision.HIGHEST)

def unit_inverse(lower):
    current_size = lower.shape[0]
    identity = jnp.eye(current_size, dtype=jnp.float32)
    result = identity - lower
    lower_power = lower
    covered = 2
    while covered < current_size:
        lower_power = matmul_f32(lower_power, lower_power)
        result = matmul_f32(result, identity + lower_power)
        covered = covered * 2
    return result

def block_terms(key_blk, value_blk, beta_blk, logd_blk):
    current_size = key_blk.shape[0]
    cumulative = jnp.cumsum(logd_blk)
    spread = cumulative[:, None] - cumulative[None, :]
    location_positions = jnp.arange(current_size)
    causal = location_positions[:, None] >= location_positions[None, :]
    strict = location_positions[:, None] > location_positions[None, :]
    decay_table = jnp.where(causal, jnp.exp(jnp.where(causal, spread, 0.0)), 0.0)
    key_beta = key_blk * beta_blk[:, None]
    lower = jnp.where(strict, matmul_f32(key_beta, key_blk.T) * decay_table, 0.0)
    inverse = unit_inverse(lower)
    update = matmul_f32(inverse, value_blk * beta_blk[:, None])
    erase = matmul_f32(inverse, key_beta * jnp.exp(cumulative)[:, None])
    key_remainder = key_blk * jnp.exp(cumulative[-1] - cumulative)[:, None]
    return (update, erase, key_remainder, jnp.exp(cumulative[-1]))

def reference(tokens, w_key, w_value, w_beta, w_decay, beta_bias, decay_rate, forgetting_increment, new_query, read_gain):
    key_raw = jnp.dot(tokens, w_key, preferred_element_type=jnp.float32).astype(jnp.bfloat16)
    value_raw = jnp.dot(tokens, w_value, preferred_element_type=jnp.float32).astype(jnp.bfloat16)
    key_wide = lax.optimization_barrier(key_raw).astype(jnp.float32).reshape(LENGTH, HEADS, DK)
    key_unit = key_wide * lax.rsqrt(lax.optimization_barrier(jnp.sum(key_wide * key_wide, axis=-1, keepdims=True)) + norm_eps)
    value_wide = lax.optimization_barrier(value_raw).astype(jnp.float32).reshape(LENGTH, HEADS, DV)
    beta = jax.nn.sigmoid(jnp.dot(tokens, w_beta, preferred_element_type=jnp.float32) + beta_bias)
    log_decay = -decay_rate * jax.nn.softplus(jnp.dot(tokens, w_decay, preferred_element_type=jnp.float32)) + forgetting_increment.T
    blocks = LENGTH // BLOCK
    key_heads = key_unit.transpose(1, 0, 2).reshape(HEADS, blocks, BLOCK, DK)
    value_heads = value_wide.transpose(1, 0, 2).reshape(HEADS, blocks, BLOCK, DV)
    beta_heads = beta.T.reshape(HEADS, blocks, BLOCK)
    logd_heads = log_decay.T.reshape(HEADS, blocks, BLOCK)
    terms = jax.vmap(jax.vmap(block_terms))(key_heads, value_heads, beta_heads, logd_heads)
    inputs = tuple((jnp.moveaxis(item, 1, 0) for item in terms))

    def advance(state, block_in):
        update, erase, key_remainder, keep = block_in
        fresh = update - jnp.einsum('hcd,hde->hce', erase, state, precision=lax.Precision.HIGHEST)
        state = keep[:, None, None] * state + jnp.einsum('hcd,hce->hde', key_remainder, fresh, precision=lax.Precision.HIGHEST)
        return (state, None)
    final_state, _ = lax.scan(advance, jnp.zeros((HEADS, DK, DV), jnp.float32), inputs)
    state_cache = final_state.astype(jnp.bfloat16)
    raw_read = lax.optimization_barrier(jnp.sum(new_query.astype(jnp.float32)[:, :, None] * state_cache.astype(jnp.float32), axis=1))
    first_read = raw_read * lax.rsqrt(lax.optimization_barrier(jnp.mean(raw_read * raw_read, axis=-1, keepdims=True)) + norm_eps) * read_gain.astype(jnp.float32)
    return (state_cache, first_read)
```

```python
import functools

import jax
import jax.numpy as jnp
from jax import lax
from jax.experimental import pallas as pl
from jax.experimental.pallas import tpu as pltpu
from jax.sharding import PartitionSpec as P

DK = 128
DV = 128
CHUNK = 128
LANES = 128
SUB = 8
norm_eps = 1e-06
MESH = pl.DeviceIdType.MESH
F32 = jnp.float32
BF16 = jnp.bfloat16


def mm(left, right):
    return jnp.dot(left.astype(BF16), right.astype(BF16), preferred_element_type=F32)


def mm_nt(left, right):
    return lax.dot_general(
        left.astype(BF16), right.astype(BF16), (((1,), (1,)), ((), ())), preferred_element_type=F32
    )


def log2(value):
    return value.bit_length() - 1


def near_rounds(n_sp):
    return 2 if n_sp == 8 else 0


def tree_shape(n_sp, heads):
    joins = log2(n_sp) - 2
    splits = min(joins, log2(heads))
    width_z = heads >> splits
    return joins, splits, width_z, 1 << (joins - splits)


def tail_pieces(features):
    return 4 if features % 1024 == 0 else 1


def body(
    n_sp,
    n_tp,
    x_hbm,
    wk_hbm,
    wv_hbm,
    wb_hbm,
    wd_hbm,
    bias_hbm,
    rate_hbm,
    finc_hbm,
    q_hbm,
    gain_hbm,
    state_out,
    read_out,
    wk,
    wv,
    wb,
    wd,
    bias_ref,
    rate_ref,
    finc_ref,
    q_ref,
    gain_ref,
    wg,
    x_ref,
    finc8,
    q_own,
    xg,
    acck,
    accv,
    accg,
    maps,
    gams,
    sendbuf,
    recvbuf,
    gsend,
    grecv,
    zsend,
    zrecv,
    gzsend,
    gzrecv,
    qslots,
    q_wide,
    fstate,
    final_ref,
    fread,
    rrecv,
    wsem,
    ready,
    own_recv,
    tok_recv,
    q_recv,
    map_recv,
    g_recv,
    z_recv,
    gz_recv,
    s_recv,
    r_recv,
):
    sp = lax.axis_index("sp")
    tp = lax.axis_index("tp")
    tokens_here, features = x_ref.shape
    heads = wk.shape[1] // DK
    chunks = tokens_here // CHUNK
    last = chunks - 1
    pieces = tail_pieces(features)
    wide = features // pieces
    parts = last + pieces
    n_y = n_tp // 2
    y = tp // 2
    core = tp % 2
    sibling = tp + 1 - 2 * core
    levels = log2(n_sp)
    rows_out = DK // n_sp
    joins, splits, width_z, copies = tree_shape(n_sp, heads)
    base = 1 << joins
    line_z = sp // base

    (map_send, z_send, s_send, r_send, tok_send, q_send, g_send, gz_send) = (
        wsem.at[pl.ds(place, 1)] for place in range(8)
    )
    barrier = pltpu.get_barrier_semaphore()

    def tell(semaphore, place):
        pl.semaphore_signal(semaphore, inc=1, device_id=place, device_id_type=MESH)

    def flip(mask):
        found = sp
        for place in range(levels):
            if (mask >> place) % 2:
                found = found + (1 - 2 * ((sp // (1 << place)) % 2)) * (1 << place)
        return found

    line = sp // 2
    lines = n_sp // 2

    def tell_near(semaphore):
        tell(semaphore, {"sp": flip(1)})

        @pl.when(line > 0)
        def _():
            tell(semaphore, {"sp": sp - 2})

        @pl.when(line < lines - 1)
        def _():
            tell(semaphore, {"sp": sp + 2})

    near_count = 1 + jnp.where(line > 0, 1, 0) + jnp.where(line < lines - 1, 1, 0)
    rounds = near_rounds(n_sp)

    for step in range(1, n_y):
        peer = ((y + step) % n_y) * 2 + core
        tell(barrier, {"tp": peer})
    tell(barrier, {"tp": sibling})
    if rounds:
        tell_near(barrier)
        greeted = n_y + near_count
    else:
        for mask in range(1, n_sp):
            tell(barrier, {"sp": flip(mask)})
        greeted = n_y + n_sp - 1

    load_x = pltpu.make_async_copy(x_hbm, x_ref, wsem.at[4])
    load_x.start()
    small = [
        pltpu.make_async_copy(source, target, wsem.at[5 + place])
        for place, (source, target) in enumerate(
            (
                (q_hbm, q_ref),
                (finc_hbm, finc_ref),
                (bias_hbm, bias_ref),
                (rate_hbm, rate_ref),
                (gain_hbm, gain_ref),
            )
        )
    ]
    loads = [
        pltpu.make_async_copy(wk_hbm, wk, wsem.at[0]),
        pltpu.make_async_copy(wv_hbm, wv, wsem.at[1]),
        pltpu.make_async_copy(wb_hbm, wb, wsem.at[2]),
        pltpu.make_async_copy(wd_hbm, wd, wsem.at[3]),
    ]
    for load in (*small, loads[2], loads[3], loads[0], loads[1]):
        load.start()

    def part_of(k):
        if isinstance(k, int) and k >= last:
            return pl.ds(last * CHUNK, CHUNK), pl.ds((k - last) * wide, wide)
        start = k * CHUNK if isinstance(k, int) else pl.multiple_of(k * CHUNK, CHUNK)
        return pl.ds(start, CHUNK), pl.ds(0, features)

    def copy_own(source):
        return pltpu.make_async_remote_copy(
            src_ref=x_ref,
            dst_ref=xg.at[source],
            send_sem=tok_send.at[0],
            recv_sem=own_recv.at[0],
            device_id={"tp": sibling},
            device_id_type=MESH,
        )

    def copy_peer(step, k):
        rows, cols = part_of(k)
        peer = ((y + step) % n_y) * 2 + core
        return pltpu.make_async_remote_copy(
            src_ref=x_ref.at[rows, cols],
            dst_ref=xg.at[tp, rows, cols],
            send_sem=tok_send.at[0],
            recv_sem=tok_recv.at[step - 1, k],
            device_id={"tp": peer},
            device_id_type=MESH,
        )

    def copy_forward(step, k):
        rows, cols = part_of(k)
        source = ((y + n_y - step) % n_y) * 2 + core
        return pltpu.make_async_remote_copy(
            src_ref=xg.at[source, rows, cols],
            dst_ref=xg.at[source, rows, cols],
            send_sem=tok_send.at[0],
            recv_sem=tok_recv.at[n_y - 2 + step, k],
            device_id={"tp": sibling},
            device_id_type=MESH,
        )

    def arrived(source, place, k):
        rows, cols = part_of(k)
        pltpu.make_async_remote_copy(
            src_ref=xg.at[source, rows, cols],
            dst_ref=xg.at[source, rows, cols],
            send_sem=tok_send.at[0],
            recv_sem=tok_recv.at[place, k],
            device_id={"tp": sibling},
            device_id_type=MESH,
        ).wait_recv()

    pl.semaphore_wait(barrier, greeted)
    load_x.wait()
    for k in range(parts):
        for step in range(1, n_y):
            copy_peer(step, k).start()
        if k == 0:
            copy_own(tp).start()
    if rounds:
        tell_near(ready.at[0])
    for load in small:
        load.wait()

    rows_q = lax.broadcasted_iota(jnp.int32, (rows_out, LANES), 0)
    lanes_q = lax.broadcasted_iota(jnp.int32, (rows_out, LANES), 1)
    place_q = jnp.where(lanes_q == rows_q + sp * rows_out, 1.0, 0.0)
    q_own[...] = jnp.zeros_like(q_own)
    q_own[0:heads, :] = mm(q_ref[...], place_q)

    lead = heads // 2
    bit0 = sp % 2
    turn = jnp.where(line_z < 2, 1, 0)

    def actual(i):
        if heads == 1:
            return i
        found = (i + (1 - bit0) * lead) % heads
        return found + turn * (1 - 2 * (found % 2)) if lead == 2 else found

    finc8[...] = jnp.zeros_like(finc8)
    for i in range(heads):
        finc8[i : i + 1, :] = finc_ref[pl.ds(actual(i), 1), :]

    total_heads = wb.shape[0]
    row_id = lax.broadcasted_iota(jnp.int32, (LANES, total_heads), 0)
    col_id = lax.broadcasted_iota(jnp.int32, (LANES, total_heads), 1)
    first_head = tp * heads
    own_head = first_head + actual(row_id % SUB)
    own = (row_id % SUB < heads) & (col_id == own_head)
    pick_b = jnp.where(own & (row_id < SUB), 1.0, 0.0)
    pick_d = jnp.where(own & (row_id >= SUB) & (row_id < 2 * SUB), 1.0, 0.0)
    loads[2].wait()
    loads[3].wait()
    depth = wg.shape[0]
    piece = 512

    def pick(step, carry):
        rows = pl.ds(pl.multiple_of(step * piece, piece), piece)
        both = mm(pick_b, wb[:, rows]) + mm(pick_d, wd[:, rows])
        wg[rows, :] = jnp.transpose(both).astype(BF16)
        return carry

    lax.fori_loop(0, depth // piece, pick, 0)
    loads[0].wait()
    loads[1].wait()

    def project(x, source, rows, first=False, start=0, size=features):
        deep = pl.ds(pl.multiple_of(source * features + start, size), size)
        for acc, weights in ((acck, wk), (accv, wv), (accg, wg)):
            part = jnp.dot(x, weights[deep, :], preferred_element_type=F32)
            acc[rows, :] = part if first else acc[rows, :] + part

    half_rows = 256 if tokens_here % 256 == 0 else CHUNK

    def own_project(step, carry):
        rows = pl.ds(pl.multiple_of(step * half_rows, half_rows), half_rows)
        project(x_ref[rows, :], tp, rows, True)
        return carry

    lax.fori_loop(0, tokens_here // half_rows, own_project, 0)
    copy_own(sibling).wait_recv()
    for step in range(1, rounds):
        pl.semaphore_wait(ready.at[step - 1], near_count)
        tell_near(ready.at[step])

    def sibling_project(step, carry):
        rows = pl.ds(pl.multiple_of(step * half_rows, half_rows), half_rows)
        project(xg[sibling, rows, :], sibling, rows)
        return carry

    lax.fori_loop(0, tokens_here // half_rows, sibling_project, 0)
    if rounds:
        pl.semaphore_wait(ready.at[rounds - 1], near_count)

    def owner_of(h, copy):
        return (1 + h % width_z) * base + h // width_z + (copy << splits)

    def copy_query(h, copy):
        owner = owner_of(h, copy)
        return pltpu.make_async_remote_copy(
            src_ref=q_own,
            dst_ref=qslots.at[sp],
            send_sem=q_send.at[0],
            recv_sem=q_recv.at[0],
            device_id={"sp": owner},
            device_id_type=MESH,
        )

    owners = [(h, copy) for h in range(heads) for copy in range(copies)]
    for h, copy in owners:

        @pl.when(sp != owner_of(h, copy))
        def _(h=h, copy=copy):
            copy_query(h, copy).start()

    row8 = lax.broadcasted_iota(jnp.int32, (SUB, total_heads), 0)
    lane8 = lax.broadcasted_iota(jnp.int32, (SUB, total_heads), 1)
    mine = (lane8 == first_head + actual(row8)) & (row8 < heads)
    bias_col = jnp.sum(jnp.where(mine, bias_ref[...], 0.0), axis=1, keepdims=True)
    rate_col = jnp.sum(jnp.where(mine, rate_ref[...], 0.0), axis=1, keepdims=True)

    maps[...] = jnp.zeros_like(maps)
    gams[...] = jnp.ones_like(gams)

    def near(step):
        return ((y + n_y - step) % n_y) * 2 + core

    def far(step):
        return ((y + n_y - step) % n_y) * 2 + 1 - core

    def gate_terms(rows):
        ri = lax.broadcasted_iota(jnp.int32, (CHUNK, CHUNK), 0)
        ci = lax.broadcasted_iota(jnp.int32, (CHUNK, CHUNK), 1)
        strict = ri > ci
        upper = jnp.where(ri <= ci, 1.0, 0.0).astype(BF16)
        gates = jnp.transpose(accg[rows, :])
        beta = jax.nn.sigmoid(gates[0:SUB, :] + bias_col)
        raw = gates[SUB : 2 * SUB, :]
        softplus = jnp.maximum(raw, 0.0) + jnp.log1p(jnp.exp(-jnp.abs(raw)))
        logd = -rate_col * softplus + finc8[:, rows]
        high = logd.astype(BF16).astype(F32)
        rest = logd - high
        middle = rest.astype(BF16).astype(F32)
        thirds = jnp.concatenate([high, middle, rest - middle], axis=0)
        sums = mm(thirds, upper)
        cum = sums[0:SUB] + sums[SUB : 2 * SUB] + sums[2 * SUB :]
        total = jnp.sum(logd, axis=1, keepdims=True)
        columns = jnp.transpose(
            jnp.concatenate(
                [
                    beta,
                    cum,
                    jnp.exp(cum),
                    jnp.exp(total - cum),
                    jnp.zeros((LANES - 4 * SUB, LANES), F32),
                ],
                axis=0,
            )
        )
        return strict, cum, columns, jnp.exp(total)

    def prepare(rows, chosen):
        found = []
        for h in chosen:
            cols = pl.ds(pl.multiple_of(actual(h) * DK, DK), DK)
            key = acck[rows, cols].astype(BF16).astype(F32)
            key = key * lax.rsqrt(jnp.sum(key * key, axis=-1, keepdims=True) + norm_eps)
            seen = mm(key, maps[h])
            erased = jnp.concatenate([seen[:, :DV], seen[:, DV:] + gams[h, 0:1, 0:1] * key], axis=1)
            found.append((key, mm_nt(key, key), erased))
        return found

    def advance(rows, terms, chosen, found=None, pause=None):
        strict, cum, columns, keep = terms
        found = prepare(rows, chosen) if found is None else found
        solved, powers, remains = [], [], []
        for h, (key, pairs, erased) in zip(chosen, found):
            cols = pl.ds(pl.multiple_of(actual(h) * DK, DK), DK)
            value = accv[rows, cols].astype(BF16).astype(F32)
            b_col = columns[:, h : h + 1]
            c_col = columns[:, SUB + h : SUB + h + 1]
            e_col = columns[:, 2 * SUB + h : 2 * SUB + h + 1]
            r_col = columns[:, 3 * SUB + h : 3 * SUB + h + 1]
            decay = jnp.exp(jnp.where(strict, c_col - cum[h : h + 1, :], 0.0))
            powers.append(jnp.where(strict, pairs * (b_col * decay), 0.0))
            gone = (b_col * e_col) * erased
            solved.append(jnp.concatenate([value * b_col - gone[:, :DV], -gone[:, DV:]], axis=1))
            remains.append(jnp.transpose(key * r_col))
        solved = [right - mm(power, right) for power, right in zip(powers, solved)]
        covered = 2
        while covered < CHUNK:
            powers = [mm(power, power) for power in powers]
            solved = [known + mm(power, known) for power, known in zip(powers, solved)]
            covered *= 2
            if covered == 16 and pause is not None:
                pause()
        for h, remain, new in zip(chosen, remains, solved):
            maps[h] = keep[h : h + 1, 0:1] * maps[h] + mm(remain, new)
            gams[h] = keep[h : h + 1, 0:1] * gams[h]

    def near_take(k):
        for step in range(1, n_y):
            arrived(near(step), step - 1, k)
            copy_forward(step, k).start()

    def far_take(k):
        for step in range(1, n_y):
            arrived(far(step), n_y - 2 + step, k)

    def take_in(side, rows):
        for step in range(1, n_y):
            project(xg[side(step), rows, :], side(step), rows)

    def chunk_step(c, carry):
        rows = pl.ds(pl.multiple_of(c * CHUNK, CHUNK), CHUNK)
        near_take(c)
        take_in(near, rows)
        far_take(c)
        take_in(far, rows)
        advance(rows, gate_terms(rows), range(heads))
        return carry

    end_rows = pl.ds(last * CHUNK, CHUNK)

    def end_project(side, place, number):
        cols = pl.ds(place * wide, number * wide)
        for step in range(1, n_y):
            project(
                xg[side(step), end_rows, cols],
                side(step),
                end_rows,
                False,
                place * wide,
                number * wide,
            )

    if pieces == 4 and last > 1:
        lax.fori_loop(0, last - 1, chunk_step, 0)
        before = last - 1
        rows = pl.ds(before * CHUNK, CHUNK)
        near_take(before)
        take_in(near, rows)

        @pl.when(core == 1)
        def _():
            near_take(last)
            near_take(last + 1)

        far_take(before)
        take_in(far, rows)

        @pl.when(core == 1)
        def _():
            near_take(last + 2)

        def pause():
            @pl.when(core == 1)
            def _():
                near_take(last + 3)

        advance(rows, gate_terms(rows), range(heads), pause=pause)

        @pl.when(core == 1)
        def _():
            end_project(near, 0, 4)
            far_take(last)
            far_take(last + 1)
            end_project(far, 0, 2)
            far_take(last + 2)
            end_project(far, 2, 1)
            far_take(last + 3)
            end_project(far, 3, 1)

        @pl.when(core == 0)
        def _():
            near_take(last)
            near_take(last + 1)
            end_project(near, 0, 2)
            near_take(last + 2)
            far_take(last)
            far_take(last + 1)
            end_project(far, 0, 2)
            end_project(near, 2, 1)
            far_take(last + 2)
            near_take(last + 3)
            far_take(last + 3)
            end_project(far, 2, 2)
            end_project(near, 3, 1)
    else:
        lax.fori_loop(0, last, chunk_step, 0)
        for place in range(pieces):
            near_take(last + place)
            end_project(near, place, 1)
        for place in range(pieces):
            far_take(last + place)
            end_project(far, place, 1)
    first_out = range(heads // 2 if heads > 1 else heads)
    end_found = prepare(end_rows, first_out)
    end_terms = gate_terms(end_rows)

    def copy_map(slot, part, partner):
        return pltpu.make_async_remote_copy(
            src_ref=sendbuf.at[slot, part],
            dst_ref=recvbuf.at[slot, part],
            send_sem=map_send.at[0],
            recv_sem=map_recv.at[slot, part],
            device_id={"sp": partner},
            device_id_type=MESH,
        )

    def copy_gamma(level, slot, number, partner):
        slots = pl.ds(slot, number)
        return pltpu.make_async_remote_copy(
            src_ref=gsend.at[slots],
            dst_ref=grecv.at[slots],
            send_sem=g_send.at[0],
            recv_sem=g_recv.at[level],
            device_id={"sp": partner},
            device_id_type=MESH,
        )

    def goal(j):
        return 1 + (turn + j) % 2 if width_z == 2 else 1

    def copy_up(j, part):
        return pltpu.make_async_remote_copy(
            src_ref=zsend.at[j, part],
            dst_ref=zrecv.at[line_z, part],
            send_sem=z_send.at[0],
            recv_sem=z_recv.at[line_z, part],
            device_id={"sp": sp % base + goal(j) * base},
            device_id_type=MESH,
        )

    def copy_up_gamma(j):
        return pltpu.make_async_remote_copy(
            src_ref=gzsend.at[j],
            dst_ref=gzrecv.at[line_z],
            send_sem=gz_send.at[0],
            recv_sem=gz_recv.at[line_z],
            device_id={"sp": sp % base + goal(j) * base},
            device_id_type=MESH,
        )

    count = heads
    offset = 0
    held = 0
    for level in range(joins):
        bit = (sp // (1 << level)) % 2
        later = bit == 1
        partner = flip(1 << level)
        split = count > 1
        half = count // 2 if split else count
        if level == 0:
            send_at, keep_at = 0, heads - half
        else:
            keep_at = held + (bit * half if split else 0)
            send_at = held + ((1 - bit) * half if split else 0)
        for j in range(half):
            if level == 0:
                gsend[j] = end_terms[3][j : j + 1, 0:1] * gams[j]
            else:
                gsend[offset + j] = gams[send_at + j]
        copy_gamma(level, offset, half, partner).start()
        if level == 0:
            advance(end_rows, end_terms, first_out, end_found)
        for j in range(half):
            slot = offset + j
            sendbuf[slot, 1] = maps[send_at + j, :, DV:].astype(BF16)
            copy_map(slot, 1, partner).start()
            sendbuf[slot, 0] = maps[send_at + j, :, :DV].astype(BF16)
            copy_map(slot, 0, partner).start()
        if level == 0 and split:
            advance(end_rows, end_terms, range(half, heads))
        top = level == joins - 1
        copy_gamma(level, offset, half, partner).wait_recv()
        if top:
            for j in range(half):
                gzsend[j] = gams[keep_at + j] * grecv[offset + j]

                @pl.when(jnp.logical_and(line_z != goal(j), line_z > 0))
                def _(j=j):
                    copy_up_gamma(j).start()

        for j in range(half):
            slot = offset + j
            own = maps[keep_at + j]
            if not split:
                own = own.astype(BF16).astype(F32)
            own_g = gams[keep_at + j]
            got_g = grecv[slot]
            left_g = jnp.where(later, own_g, got_g)[0:1, 0:1]
            right_g = jnp.where(later, got_g, own_g)[0:1, 0:1]
            gams[keep_at + j] = own_g * got_g
            copy_map(slot, 1, partner).wait_recv()
            got = recvbuf[slot, 1].astype(F32)
            left = jnp.where(later, own[:, DV:], got)
            right = jnp.where(later, got, own[:, DV:])
            joined = left_g * right + mm(left, right) + right_g * left
            maps[keep_at + j, :, DV:] = joined
            if top:
                zsend[j, 1] = joined.astype(BF16)

                @pl.when(jnp.logical_and(line_z != goal(j), line_z > 0))
                def _(j=j):
                    copy_up(j, 1).start()

            copy_map(slot, 0, partner).wait_recv()
            got = recvbuf[slot, 0].astype(F32)
            left_b = jnp.where(later, own[:, :DV], got)
            right_b = jnp.where(later, got, own[:, :DV])
            joined = left_g * right_b + mm(left, right_b) + left_b
            maps[keep_at + j, :, :DV] = joined
            if top:
                zsend[j, 0] = joined.astype(BF16)

                @pl.when(line_z != goal(j))
                def _(j=j):
                    copy_up(j, 0).start()

        offset += half
        count = half
        held = keep_at

    def copy_state(mask, h):
        target = flip(mask)
        return pltpu.make_async_remote_copy(
            src_ref=fstate.at[target],
            dst_ref=state_out.at[h],
            send_sem=s_send.at[0],
            recv_sem=s_recv.at[0],
            device_id={"sp": target},
            device_id_type=MESH,
        )

    def copy_read(mask, h):
        target = flip(mask)
        return pltpu.make_async_remote_copy(
            src_ref=fread,
            dst_ref=rrecv.at[h],
            send_sem=r_send.at[0],
            recv_sem=r_recv.at[0],
            device_id={"sp": target},
            device_id_type=MESH,
        )

    def settle(ref, sent, landed):
        return pltpu.make_async_remote_copy(
            src_ref=ref,
            dst_ref=ref,
            send_sem=sent.at[0],
            recv_sem=landed,
            device_id={"sp": sp},
            device_id_type=MESH,
        )

    free = [1 << place for place in range(levels) if place < splits or place >= joins]
    masks = [0]
    for place in reversed(free):
        masks = [mask + more for more in (place, 0) for mask in masks]
    masks = [mask for mask in sorted(masks, key=lambda mask: (mask // base % 4 != 2, -(mask % base))) if mask]
    is_owner = jnp.logical_and(line_z >= 1, line_z <= width_z)
    my_head = (sp % (1 << splits)) * width_z + line_z - 1
    own_at = held + width_z - 1

    @pl.when(is_owner)
    def _():
        settle(qslots.at[pl.ds(0, n_sp - 1)], q_send, q_recv.at[0]).wait_recv()
        qslots[sp] = q_own[...]
        query = jnp.sum(qslots[...], axis=0)
        row_head = lax.broadcasted_iota(jnp.int32, (SUB, DK), 0)
        mine_q = jnp.sum(jnp.where(row_head == my_head, query, 0.0), axis=0, keepdims=True)
        q_wide[...] = jnp.transpose(jnp.broadcast_to(mine_q, (LANES, DK)))

    def follow(line, state):
        settle(gzrecv.at[line], gz_send, gz_recv.at[line]).wait_recv()
        settle(zrecv.at[line, 1], z_send, z_recv.at[line, 1]).wait_recv()
        moved = gzrecv[line, 0:1, 0:1] * state + mm(zrecv[line, 1], state)
        settle(zrecv.at[line, 0], z_send, z_recv.at[line, 0]).wait_recv()
        return moved + zrecv[line, 0].astype(F32)

    def keep_own(state):
        own = maps[own_at]
        return gams[own_at, 0:1, 0:1] * state + mm(own[:, DV:], state) + own[:, :DV]

    for g in range(1, 1 + width_z):

        @pl.when(line_z == g)
        def _(g=g):
            settle(zrecv.at[0, 0], z_send, z_recv.at[0, 0]).wait_recv()
            state = zrecv[0, 0].astype(F32)
            for line in range(1, 4):
                state = keep_own(state) if line == g else follow(line, state)
            final_ref[...] = state

    @pl.when(is_owner)
    def _():
        final = final_ref[...].astype(BF16)
        for j in range(n_sp):
            fstate[j] = final[j * rows_out : (j + 1) * rows_out, :]
        for mask in masks:
            copy_state(mask, my_head).start()
        raw_read = jnp.sum(final.astype(F32) * q_wide[...], axis=0, keepdims=True)
        read = (
            raw_read
            * lax.rsqrt(jnp.mean(raw_read * raw_read, axis=-1, keepdims=True) + norm_eps)
            * gain_ref[...].astype(F32)
        )
        fread[...] = jnp.broadcast_to(read, fread.shape)
        for mask in masks:
            copy_read(mask, my_head).start()
        state_out[my_head] = fstate[sp]
        rrecv[my_head] = fread[...]

    def both_ways(act):
        for owns, number in ((True, -1), (False, 0)):

            @pl.when(is_owner == owns)
            def _(number=number):
                act(number)

    settle(xg.at[pl.ds(0, 2 * n_y - 1)], tok_send, own_recv.at[0]).wait_send()
    settle(sendbuf, map_send, map_recv.at[0, 0]).wait_send()
    settle(gsend, g_send, g_recv.at[0]).wait_send()
    both_ways(
        lambda number: settle(
            qslots.at[pl.ds(0, len(owners) + number)], q_send, q_recv.at[0]
        ).wait_send()
    )

    @pl.when(line_z == 0)
    def _():
        settle(zsend.at[:, 0], z_send, z_recv.at[0, 0]).wait_send()

    for line in range(1, 4):
        number = width_z - 1 if line <= width_z else width_z
        if number:

            @pl.when(line_z == line)
            def _(number=number):
                settle(zsend.at[pl.ds(0, number)], z_send, z_recv.at[0, 0]).wait_send()
                settle(gzsend.at[pl.ds(0, number)], gz_send, gz_recv.at[0]).wait_send()

    def states_in(number):
        if heads + number:
            held_rows = state_out.at[pl.ds(0, heads + number)]
            settle(held_rows, s_send, s_recv.at[0]).wait_recv()
            settle(rrecv.at[pl.ds(0, heads + number)], r_send, r_recv.at[0]).wait_recv()

    both_ways(states_in)
    for h in range(heads):
        read_out[h : h + 1, :] = rrecv[h, 0:1, :]

    @pl.when(is_owner)
    def _():
        settle(fstate.at[pl.ds(0, len(masks))], s_send, s_recv.at[0]).wait_send()
        settle(qslots.at[pl.ds(0, len(masks))], r_send, r_recv.at[0]).wait_send()


def hand_over(state_ref, read_ref, state_out, read_out):
    state_out[...] = state_ref[...]
    read_out[...] = read_ref[...]


def per_device(
    n_sp,
    n_tp,
    tokens,
    w_key,
    w_value,
    w_beta,
    w_decay,
    beta_bias,
    decay_rate,
    forgetting_increment,
    new_query,
    read_gain,
):
    tokens_here, features = tokens.shape
    depth, width = w_key.shape
    heads = width // DK
    parts = tokens_here // CHUNK - 1 + tail_pieces(features)
    rows_out = DK // n_sp
    n_y = n_tp // 2
    total_heads = w_beta.shape[1]
    joins, splits, width_z, copies = tree_shape(n_sp, heads)
    slots = 0
    count = heads
    for _ in range(joins):
        count = max(count // 2, 1)
        slots += count
    vmem = pl.BlockSpec(memory_space=pltpu.VMEM)
    hbm = pl.BlockSpec(memory_space=pl.ANY)
    dma = pltpu.SemaphoreType.DMA
    state, read = pl.pallas_call(
        functools.partial(body, n_sp, n_tp),
        name="delta_state",
        out_shape=(
            pltpu.VMEM((heads, rows_out, DV), BF16),
            pltpu.VMEM((heads, DV), F32),
        ),
        in_specs=[hbm] * 10,
        out_specs=(vmem, vmem),
        scratch_shapes=[
            pltpu.VMEM((depth, width), BF16),
            pltpu.VMEM((depth, width), BF16),
            pltpu.VMEM(w_beta.shape[::-1], BF16),
            pltpu.VMEM(w_decay.shape[::-1], BF16),
            pltpu.VMEM((1, total_heads), F32),
            pltpu.VMEM((1, total_heads), F32),
            pltpu.VMEM(forgetting_increment.shape, F32),
            pltpu.VMEM(new_query.shape, BF16),
            pltpu.VMEM((1, DV), BF16),
            pltpu.VMEM((depth, LANES), BF16),
            pltpu.VMEM((tokens_here, features), BF16),
            pltpu.VMEM((SUB, tokens_here), F32),
            pltpu.VMEM((SUB, DK), F32),
            pltpu.VMEM((n_tp, tokens_here, features), BF16),
            pltpu.VMEM((tokens_here, width), F32),
            pltpu.VMEM((tokens_here, width), F32),
            pltpu.VMEM((tokens_here, LANES), F32),
            pltpu.VMEM((heads, DK, DV + DK), F32),
            pltpu.VMEM((heads, SUB, LANES), F32),
            pltpu.VMEM((slots, 2, DK, DV), BF16),
            pltpu.VMEM((slots, 2, DK, DV), BF16),
            pltpu.VMEM((slots, SUB, LANES), F32),
            pltpu.VMEM((slots, SUB, LANES), F32),
            pltpu.VMEM((width_z, 2, DK, DV), BF16),
            pltpu.VMEM((4, 2, DK, DV), BF16),
            pltpu.VMEM((width_z, SUB, LANES), F32),
            pltpu.VMEM((4, SUB, LANES), F32),
            pltpu.VMEM((n_sp, SUB, DK), F32),
            pltpu.VMEM((DK, LANES), F32),
            pltpu.VMEM((n_sp, rows_out, DV), BF16),
            pltpu.VMEM((DK, DV), F32),
            pltpu.VMEM((SUB, DV), F32),
            pltpu.VMEM((heads, SUB, DV), F32),
            dma((10,)),
            pltpu.SemaphoreType.REGULAR((max(near_rounds(n_sp), 1),)),
            dma((1,)),
            dma((2 * (n_y - 1), parts)),
            dma((1,)),
            dma((slots, 2)),
            dma((joins,)),
            dma((4, 2)),
            dma((4,)),
            dma((1,)),
            dma((1,)),
        ],
        compiler_params=pltpu.CompilerParams(
            collective_id=0, has_side_effects=True, vmem_limit_bytes=63 * 1024 * 1024
        ),
    )(
        tokens,
        w_key,
        w_value,
        w_beta.T,
        w_decay.T,
        beta_bias[None, :],
        decay_rate[None, :],
        forgetting_increment,
        new_query,
        read_gain[None, :],
    )
    return pl.pallas_call(
        hand_over,
        name="hand_over",
        out_shape=(
            jax.ShapeDtypeStruct(state.shape, state.dtype),
            jax.ShapeDtypeStruct(read.shape, read.dtype),
        ),
        in_specs=[vmem, vmem],
        out_specs=(vmem, vmem),
    )(
        pltpu.with_memory_space_constraint(state, pltpu.VMEM),
        pltpu.with_memory_space_constraint(read, pltpu.VMEM),
    )


def solution(mesh):
    return jax.shard_map(
        functools.partial(per_device, mesh.shape["sp"], mesh.shape["tp"]),
        mesh=mesh,
        in_specs=(
            P("sp", "tp"),
            P(None, "tp"),
            P(None, "tp"),
            P(),
            P(),
            P(),
            P(),
            P("tp", "sp"),
            P("tp", "sp"),
            P(),
        ),
        out_specs=(P("tp", "sp", None), P("tp", None)),
        check_vma=False,
    )
```

```python
import functools

import jax
import jax.numpy as jnp
from jax import lax
from jax.experimental import pallas as pl
from jax.experimental.pallas import tpu as pltpu
from jax.sharding import PartitionSpec as P

DK = 128
DV = 128
CHUNK = 128
LANES = 128
SUB = 8
norm_eps = 1e-06
MESH = pl.DeviceIdType.MESH
F32 = jnp.float32
BF16 = jnp.bfloat16


def mm(left, right):
    return jnp.dot(left.astype(BF16), right.astype(BF16), preferred_element_type=F32)


def mm_nt(left, right):
    return lax.dot_general(
        left.astype(BF16), right.astype(BF16), (((1,), (1,)), ((), ())), preferred_element_type=F32
    )


def log2(value):
    return value.bit_length() - 1


def near_rounds(n_sp):
    return 3 if n_sp == 8 else 0


def tree_shape(n_sp, heads):
    joins = log2(n_sp) - 2
    splits = min(joins, log2(heads))
    width_z = heads >> splits
    return joins, splits, width_z, 1 << (joins - splits)


def tail_pieces(features):
    return 4 if features % 1024 == 0 else 1


def body(
    n_sp,
    n_tp,
    x_hbm,
    wk_hbm,
    wv_hbm,
    wb_hbm,
    wd_hbm,
    bias_hbm,
    rate_hbm,
    finc_hbm,
    q_hbm,
    gain_hbm,
    state_out,
    read_out,
    wk,
    wv,
    wb,
    wd,
    bias_ref,
    rate_ref,
    finc_ref,
    q_ref,
    gain_ref,
    wg,
    x_ref,
    finc8,
    q_own,
    xg,
    acck,
    accv,
    accg,
    maps,
    gams,
    sendbuf,
    recvbuf,
    gsend,
    grecv,
    zsend,
    zrecv,
    gzsend,
    gzrecv,
    qslots,
    q_wide,
    fstate,
    final_ref,
    srecv,
    late_out,
    late_in,
    wsem,
    ready,
    own_recv,
    tok_recv,
    q_recv,
    map_recv,
    g_recv,
    z_recv,
    gz_recv,
    s_recv,
    l_recv,
):
    sp = lax.axis_index("sp")
    tp = lax.axis_index("tp")
    tokens_here, features = x_ref.shape
    heads = wk.shape[1] // DK
    chunks = tokens_here // CHUNK
    last = chunks - 1
    pieces = tail_pieces(features)
    wide = features // pieces
    parts = last + pieces
    n_y = n_tp // 2
    y = tp // 2
    core = tp % 2
    sibling = tp + 1 - 2 * core
    levels = log2(n_sp)
    rows_out = DK // n_sp
    joins, splits, width_z, copies = tree_shape(n_sp, heads)
    base = 1 << joins
    line_z = sp // base

    (map_send, z_send, s_send, l_send, tok_send, q_send, g_send, gz_send) = (
        wsem.at[pl.ds(place, 1)] for place in range(8)
    )
    barrier = pltpu.get_barrier_semaphore()

    def tell(semaphore, place):
        pl.semaphore_signal(semaphore, inc=1, device_id=place, device_id_type=MESH)

    def flip(mask):
        found = sp
        for place in range(levels):
            if (mask >> place) % 2:
                found = found + (1 - 2 * ((sp // (1 << place)) % 2)) * (1 << place)
        return found

    line = sp // 2
    lines = n_sp // 2

    def tell_near(semaphore):
        tell(semaphore, {"sp": flip(1)})

        @pl.when(line > 0)
        def _():
            tell(semaphore, {"sp": sp - 2})

        @pl.when(line < lines - 1)
        def _():
            tell(semaphore, {"sp": sp + 2})

    near_count = 1 + jnp.where(line > 0, 1, 0) + jnp.where(line < lines - 1, 1, 0)
    rounds = near_rounds(n_sp)

    for step in range(1, n_y):
        peer = ((y + step) % n_y) * 2 + core
        tell(barrier, {"tp": peer})
    tell(barrier, {"tp": sibling})
    if rounds:
        tell_near(barrier)
        greeted = n_y + near_count
    else:
        for mask in range(1, n_sp):
            tell(barrier, {"sp": flip(mask)})
        greeted = n_y + n_sp - 1

    load_x = pltpu.make_async_copy(x_hbm, x_ref, wsem.at[4])
    load_x.start()
    small = [
        pltpu.make_async_copy(source, target, wsem.at[5 + place])
        for place, (source, target) in enumerate(
            (
                (q_hbm, q_ref),
                (finc_hbm, finc_ref),
                (bias_hbm, bias_ref),
                (rate_hbm, rate_ref),
                (gain_hbm, gain_ref),
            )
        )
    ]
    loads = [
        pltpu.make_async_copy(wk_hbm, wk, wsem.at[0]),
        pltpu.make_async_copy(wv_hbm, wv, wsem.at[1]),
        pltpu.make_async_copy(wb_hbm, wb, wsem.at[2]),
        pltpu.make_async_copy(wd_hbm, wd, wsem.at[3]),
    ]
    for load in (*small, loads[2], loads[3], loads[0], loads[1]):
        load.start()

    def part_of(k):
        if isinstance(k, int) and k >= last:
            return pl.ds(last * CHUNK, CHUNK), pl.ds((k - last) * wide, wide)
        start = k * CHUNK if isinstance(k, int) else pl.multiple_of(k * CHUNK, CHUNK)
        return pl.ds(start, CHUNK), pl.ds(0, features)

    def copy_own(source):
        return pltpu.make_async_remote_copy(
            src_ref=x_ref,
            dst_ref=xg.at[source],
            send_sem=tok_send.at[0],
            recv_sem=own_recv.at[0],
            device_id={"tp": sibling},
            device_id_type=MESH,
        )

    def copy_peer(step, k):
        rows, cols = part_of(k)
        peer = ((y + step) % n_y) * 2 + core
        return pltpu.make_async_remote_copy(
            src_ref=x_ref.at[rows, cols],
            dst_ref=xg.at[tp, rows, cols],
            send_sem=tok_send.at[0],
            recv_sem=tok_recv.at[step - 1, k],
            device_id={"tp": peer},
            device_id_type=MESH,
        )

    def copy_forward(step, k):
        rows, cols = part_of(k)
        source = ((y + n_y - step) % n_y) * 2 + core
        return pltpu.make_async_remote_copy(
            src_ref=xg.at[source, rows, cols],
            dst_ref=xg.at[source, rows, cols],
            send_sem=tok_send.at[0],
            recv_sem=tok_recv.at[n_y - 2 + step, k],
            device_id={"tp": sibling},
            device_id_type=MESH,
        )

    def arrived(source, place, k):
        rows, cols = part_of(k)
        pltpu.make_async_remote_copy(
            src_ref=xg.at[source, rows, cols],
            dst_ref=xg.at[source, rows, cols],
            send_sem=tok_send.at[0],
            recv_sem=tok_recv.at[place, k],
            device_id={"tp": sibling},
            device_id_type=MESH,
        ).wait_recv()

    pl.semaphore_wait(barrier, greeted)
    load_x.wait()
    for k in range(parts):
        for step in range(1, n_y):
            copy_peer(step, k).start()
        if k == 0:
            copy_own(tp).start()
    if rounds:
        tell_near(ready.at[0])
    for load in small:
        load.wait()

    rows_q = lax.broadcasted_iota(jnp.int32, (rows_out, LANES), 0)
    lanes_q = lax.broadcasted_iota(jnp.int32, (rows_out, LANES), 1)
    place_q = jnp.where(lanes_q == rows_q + sp * rows_out, 1.0, 0.0)
    q_own[...] = jnp.zeros_like(q_own)
    q_own[0:heads, :] = mm(q_ref[...], place_q)

    lead = heads // 2
    bit0 = sp % 2
    turn = jnp.where(line_z < 2, 1, 0)

    def actual(i):
        if heads == 1:
            return i
        found = (i + (1 - bit0) * lead) % heads
        return found + turn * (1 - 2 * (found % 2)) if lead == 2 else found

    finc8[...] = jnp.zeros_like(finc8)
    for i in range(heads):
        finc8[i : i + 1, :] = finc_ref[pl.ds(actual(i), 1), :]

    total_heads = wb.shape[0]
    row_id = lax.broadcasted_iota(jnp.int32, (LANES, total_heads), 0)
    col_id = lax.broadcasted_iota(jnp.int32, (LANES, total_heads), 1)
    first_head = tp * heads
    own_head = first_head + actual(row_id % SUB)
    own = (row_id % SUB < heads) & (col_id == own_head)
    pick_b = jnp.where(own & (row_id < SUB), 1.0, 0.0)
    pick_d = jnp.where(own & (row_id >= SUB) & (row_id < 2 * SUB), 1.0, 0.0)
    loads[2].wait()
    loads[3].wait()
    depth = wg.shape[0]
    piece = 512

    def pick(step, carry):
        rows = pl.ds(pl.multiple_of(step * piece, piece), piece)
        both = mm(pick_b, wb[:, rows]) + mm(pick_d, wd[:, rows])
        wg[rows, :] = jnp.transpose(both).astype(BF16)
        return carry

    lax.fori_loop(0, depth // piece, pick, 0)
    loads[0].wait()
    loads[1].wait()

    def project(x, source, rows, first=False, start=0, size=features):
        deep = pl.ds(pl.multiple_of(source * features + start, size), size)
        for acc, weights in ((acck, wk), (accv, wv), (accg, wg)):
            part = jnp.dot(x, weights[deep, :], preferred_element_type=F32)
            acc[rows, :] = part if first else acc[rows, :] + part

    half_rows = 256 if tokens_here % 256 == 0 else CHUNK

    def own_project(step, carry):
        rows = pl.ds(pl.multiple_of(step * half_rows, half_rows), half_rows)
        project(x_ref[rows, :], tp, rows, True)
        return carry

    lax.fori_loop(0, tokens_here // half_rows, own_project, 0)
    copy_own(sibling).wait_recv()
    for step in range(1, rounds):
        pl.semaphore_wait(ready.at[step - 1], near_count)
        tell_near(ready.at[step])

    def sibling_project(step, carry):
        rows = pl.ds(pl.multiple_of(step * half_rows, half_rows), half_rows)
        project(xg[sibling, rows, :], sibling, rows)
        return carry

    lax.fori_loop(0, tokens_here // half_rows, sibling_project, 0)
    if rounds:
        pl.semaphore_wait(ready.at[rounds - 1], near_count)

    lanes_of = 1 << splits

    def reader_of(h, copy):
        if h < heads:
            return (1 + h % width_z) * base + h // width_z + (copy << splits)
        return 3 * base + h - heads + (copy << splits)

    def copy_query(h, copy):
        owner = reader_of(h, copy)
        return pltpu.make_async_remote_copy(
            src_ref=q_own,
            dst_ref=qslots.at[sp],
            send_sem=q_send.at[0],
            recv_sem=q_recv.at[0],
            device_id={"sp": owner},
            device_id_type=MESH,
        )

    readers = [(h, copy) for h in range(heads + lanes_of) for copy in range(copies)]
    for h, copy in readers:

        @pl.when(sp != reader_of(h, copy))
        def _(h=h, copy=copy):
            copy_query(h, copy).start()

    row8 = lax.broadcasted_iota(jnp.int32, (SUB, total_heads), 0)
    lane8 = lax.broadcasted_iota(jnp.int32, (SUB, total_heads), 1)
    mine = (lane8 == first_head + actual(row8)) & (row8 < heads)
    bias_col = jnp.sum(jnp.where(mine, bias_ref[...], 0.0), axis=1, keepdims=True)
    rate_col = jnp.sum(jnp.where(mine, rate_ref[...], 0.0), axis=1, keepdims=True)

    maps[...] = jnp.zeros_like(maps)
    gams[...] = jnp.ones_like(gams)

    def near(step):
        return ((y + n_y - step) % n_y) * 2 + core

    def far(step):
        return ((y + n_y - step) % n_y) * 2 + 1 - core

    def gate_terms(rows):
        ri = lax.broadcasted_iota(jnp.int32, (CHUNK, CHUNK), 0)
        ci = lax.broadcasted_iota(jnp.int32, (CHUNK, CHUNK), 1)
        strict = ri > ci
        upper = jnp.where(ri <= ci, 1.0, 0.0).astype(BF16)
        gates = jnp.transpose(accg[rows, :])
        beta = jax.nn.sigmoid(gates[0:SUB, :] + bias_col)
        raw = gates[SUB : 2 * SUB, :]
        softplus = jnp.maximum(raw, 0.0) + jnp.log1p(jnp.exp(-jnp.abs(raw)))
        logd = -rate_col * softplus + finc8[:, rows]
        high = logd.astype(BF16).astype(F32)
        rest = logd - high
        middle = rest.astype(BF16).astype(F32)
        thirds = jnp.concatenate([high, middle, rest - middle], axis=0)
        sums = mm(thirds, upper)
        cum = sums[0:SUB] + sums[SUB : 2 * SUB] + sums[2 * SUB :]
        total = jnp.sum(logd, axis=1, keepdims=True)
        columns = jnp.transpose(
            jnp.concatenate(
                [
                    beta,
                    cum,
                    jnp.exp(cum),
                    jnp.exp(total - cum),
                    jnp.zeros((LANES - 4 * SUB, LANES), F32),
                ],
                axis=0,
            )
        )
        return strict, cum, columns, jnp.exp(total)

    def prepare(rows, chosen):
        found = []
        for h in chosen:
            cols = pl.ds(pl.multiple_of(actual(h) * DK, DK), DK)
            key = acck[rows, cols].astype(BF16).astype(F32)
            key = key * lax.rsqrt(jnp.sum(key * key, axis=-1, keepdims=True) + norm_eps)
            seen = mm(key, maps[h])
            erased = jnp.concatenate([seen[:, :DV], seen[:, DV:] + gams[h, 0:1, 0:1] * key], axis=1)
            found.append((key, mm_nt(key, key), erased))
        return found

    def advance(rows, terms, chosen, found=None, pause=None):
        strict, cum, columns, keep = terms
        found = prepare(rows, chosen) if found is None else found
        solved, powers, remains = [], [], []
        for h, (key, pairs, erased) in zip(chosen, found):
            cols = pl.ds(pl.multiple_of(actual(h) * DK, DK), DK)
            value = accv[rows, cols].astype(BF16).astype(F32)
            b_col = columns[:, h : h + 1]
            c_col = columns[:, SUB + h : SUB + h + 1]
            e_col = columns[:, 2 * SUB + h : 2 * SUB + h + 1]
            r_col = columns[:, 3 * SUB + h : 3 * SUB + h + 1]
            decay = jnp.exp(jnp.where(strict, c_col - cum[h : h + 1, :], 0.0))
            powers.append(jnp.where(strict, pairs * (b_col * decay), 0.0))
            gone = (b_col * e_col) * erased
            solved.append(jnp.concatenate([value * b_col - gone[:, :DV], -gone[:, DV:]], axis=1))
            remains.append(jnp.transpose(key * r_col))
        solved = [right - mm(power, right) for power, right in zip(powers, solved)]
        covered = 2
        while covered < CHUNK:
            powers = [mm(power, power) for power in powers]
            solved = [known + mm(power, known) for power, known in zip(powers, solved)]
            covered *= 2
            if covered == 16 and pause is not None:
                pause()
        for h, remain, new in zip(chosen, remains, solved):
            maps[h] = keep[h : h + 1, 0:1] * maps[h] + mm(remain, new)
            gams[h] = keep[h : h + 1, 0:1] * gams[h]

    def near_take(k):
        for step in range(1, n_y):
            arrived(near(step), step - 1, k)
            copy_forward(step, k).start()

    def far_take(k):
        for step in range(1, n_y):
            arrived(far(step), n_y - 2 + step, k)

    def take_in(side, rows):
        for step in range(1, n_y):
            project(xg[side(step), rows, :], side(step), rows)

    def chunk_step(c, carry):
        rows = pl.ds(pl.multiple_of(c * CHUNK, CHUNK), CHUNK)
        near_take(c)
        take_in(near, rows)
        far_take(c)
        take_in(far, rows)
        advance(rows, gate_terms(rows), range(heads))
        return carry

    end_rows = pl.ds(last * CHUNK, CHUNK)

    def end_project(side, place, number):
        cols = pl.ds(place * wide, number * wide)
        for step in range(1, n_y):
            project(
                xg[side(step), end_rows, cols],
                side(step),
                end_rows,
                False,
                place * wide,
                number * wide,
            )

    if pieces == 4 and last > 1:
        lax.fori_loop(0, last - 1, chunk_step, 0)
        before = last - 1
        rows = pl.ds(before * CHUNK, CHUNK)
        near_take(before)
        take_in(near, rows)

        @pl.when(core == 1)
        def _():
            near_take(last)
            near_take(last + 1)

        far_take(before)
        take_in(far, rows)

        @pl.when(core == 1)
        def _():
            near_take(last + 2)

        def pause():
            @pl.when(core == 1)
            def _():
                near_take(last + 3)

        advance(rows, gate_terms(rows), range(heads), pause=pause)

        @pl.when(core == 1)
        def _():
            end_project(near, 0, 4)
            far_take(last)
            far_take(last + 1)
            end_project(far, 0, 2)
            far_take(last + 2)
            far_take(last + 3)
            end_project(far, 2, 2)

        @pl.when(core == 0)
        def _():
            near_take(last)
            near_take(last + 1)
            end_project(near, 0, 2)
            near_take(last + 2)
            far_take(last)
            far_take(last + 1)
            end_project(far, 0, 2)
            end_project(near, 2, 1)
            far_take(last + 2)
            near_take(last + 3)
            far_take(last + 3)
            end_project(far, 2, 2)
            end_project(near, 3, 1)
    else:
        lax.fori_loop(0, last, chunk_step, 0)
        for place in range(pieces):
            near_take(last + place)
            end_project(near, place, 1)
        for place in range(pieces):
            far_take(last + place)
            end_project(far, place, 1)
    first_out = range(heads // 2 if heads > 1 else heads)
    end_found = prepare(end_rows, first_out)
    end_terms = gate_terms(end_rows)

    def copy_map(slot, part, partner):
        return pltpu.make_async_remote_copy(
            src_ref=sendbuf.at[slot, part],
            dst_ref=recvbuf.at[slot, part],
            send_sem=map_send.at[0],
            recv_sem=map_recv.at[slot, part],
            device_id={"sp": partner},
            device_id_type=MESH,
        )

    def copy_gamma(level, slot, number, partner):
        slots = pl.ds(slot, number)
        return pltpu.make_async_remote_copy(
            src_ref=gsend.at[slots],
            dst_ref=grecv.at[slots],
            send_sem=g_send.at[0],
            recv_sem=g_recv.at[level],
            device_id={"sp": partner},
            device_id_type=MESH,
        )

    def goal(j):
        return 1 + (turn + j) % 2 if width_z == 2 else 1

    def copy_up(j, part):
        return pltpu.make_async_remote_copy(
            src_ref=zsend.at[j, part],
            dst_ref=zrecv.at[line_z, part],
            send_sem=z_send.at[0],
            recv_sem=z_recv.at[line_z, part],
            device_id={"sp": sp % base + goal(j) * base},
            device_id_type=MESH,
        )

    def copy_up_gamma(j):
        return pltpu.make_async_remote_copy(
            src_ref=gzsend.at[j],
            dst_ref=gzrecv.at[line_z],
            send_sem=gz_send.at[0],
            recv_sem=gz_recv.at[line_z],
            device_id={"sp": sp % base + goal(j) * base},
            device_id_type=MESH,
        )

    count = heads
    offset = 0
    held = 0
    for level in range(joins):
        bit = (sp // (1 << level)) % 2
        later = bit == 1
        partner = flip(1 << level)
        split = count > 1
        half = count // 2 if split else count
        if level == 0:
            send_at, keep_at = 0, heads - half
        else:
            keep_at = held + (bit * half if split else 0)
            send_at = held + ((1 - bit) * half if split else 0)
        for j in range(half):
            if level == 0:
                gsend[j] = end_terms[3][j : j + 1, 0:1] * gams[j]
            else:
                gsend[offset + j] = gams[send_at + j]
        copy_gamma(level, offset, half, partner).start()
        if level == 0:
            advance(end_rows, end_terms, first_out, end_found)
        for j in range(half):
            slot = offset + j
            sendbuf[slot, 1] = maps[send_at + j, :, DV:].astype(BF16)
            copy_map(slot, 1, partner).start()
            sendbuf[slot, 0] = maps[send_at + j, :, :DV].astype(BF16)
            copy_map(slot, 0, partner).start()
        if level == 0 and split:
            advance(end_rows, end_terms, range(half, heads))
        top = level == joins - 1
        copy_gamma(level, offset, half, partner).wait_recv()
        if top:
            for j in range(half):
                gzsend[j] = gams[keep_at + j] * grecv[offset + j]

                @pl.when(jnp.logical_and(line_z != goal(j), line_z > 0))
                def _(j=j):
                    copy_up_gamma(j).start()

        for j in range(half):
            slot = offset + j
            own = maps[keep_at + j]
            if not split:
                own = own.astype(BF16).astype(F32)
            own_g = gams[keep_at + j]
            got_g = grecv[slot]
            left_g = jnp.where(later, own_g, got_g)[0:1, 0:1]
            right_g = jnp.where(later, got_g, own_g)[0:1, 0:1]
            gams[keep_at + j] = own_g * got_g
            copy_map(slot, 1, partner).wait_recv()
            got = recvbuf[slot, 1].astype(F32)
            left = jnp.where(later, own[:, DV:], got)
            right = jnp.where(later, got, own[:, DV:])
            joined = left_g * right + mm(left, right) + right_g * left
            maps[keep_at + j, :, DV:] = joined
            if top:
                zsend[j, 1] = joined.astype(BF16)

                @pl.when(jnp.logical_and(line_z != goal(j), line_z > 0))
                def _(j=j):
                    copy_up(j, 1).start()

            copy_map(slot, 0, partner).wait_recv()
            got = recvbuf[slot, 0].astype(F32)
            left_b = jnp.where(later, own[:, :DV], got)
            right_b = jnp.where(later, got, own[:, :DV])
            joined = left_g * right_b + mm(left, right_b) + left_b
            maps[keep_at + j, :, :DV] = joined
            if top:
                zsend[j, 0] = joined.astype(BF16)

                @pl.when(jnp.logical_and(line_z != goal(j), line_z < 3))
                def _(j=j):
                    copy_up(j, 0).start()

        offset += half
        count = half
        held = keep_at

    def copy_state(mask, h):
        target = flip(mask)
        return pltpu.make_async_remote_copy(
            src_ref=fstate.at[target],
            dst_ref=srecv.at[h],
            send_sem=s_send.at[0],
            recv_sem=s_recv.at[0],
            device_id={"sp": target},
            device_id_type=MESH,
        )

    def copy_late(mask):
        target = flip(mask)
        return pltpu.make_async_remote_copy(
            src_ref=late_out.at[target],
            dst_ref=late_in.at[sp % lanes_of],
            send_sem=l_send.at[0],
            recv_sem=l_recv.at[0],
            device_id={"sp": target},
            device_id_type=MESH,
        )

    def settle(ref, sent, landed):
        return pltpu.make_async_remote_copy(
            src_ref=ref,
            dst_ref=ref,
            send_sem=sent.at[0],
            recv_sem=landed,
            device_id={"sp": sp},
            device_id_type=MESH,
        )

    free = [1 << place for place in range(levels) if place < splits or place >= joins]
    masks = [0]
    for place in reversed(free):
        masks = [mask + more for more in (place, 0) for mask in masks]
    masks = [mask for mask in sorted(masks, key=lambda mask: (mask // base % 4 != 2, -(mask % base))) if mask]
    is_owner = jnp.logical_and(line_z >= 1, line_z <= width_z)
    is_last = line_z == 3
    reads_query = jnp.logical_or(is_owner, is_last)
    my_lane = sp % lanes_of
    my_head = my_lane * width_z + line_z - 1
    own_at = held + width_z - 1
    space = srecv.shape[1] - SUB
    row_head = lax.broadcasted_iota(jnp.int32, (SUB, DK), 0)

    @pl.when(reads_query)
    def _():
        settle(qslots.at[pl.ds(0, n_sp - 1)], q_send, q_recv.at[0]).wait_recv()
        qslots[sp] = q_own[...]

    @pl.when(is_last)
    def _():
        query = jnp.sum(qslots[...], axis=0)
        for i in range(width_z):
            part = maps[held + i, :, :DV]
            reads = mm(query, part)
            wanted = row_head == my_lane * width_z + i
            line_read = jnp.sum(jnp.where(wanted, reads, 0.0), axis=0, keepdims=True)
            for j in range(n_sp):
                late_out[j, i * space : i * space + rows_out, :] = part[
                    j * rows_out : (j + 1) * rows_out, :
                ]
                late_out[j, width_z * space + i : width_z * space + i + 1, :] = line_read
        for mask in masks:
            copy_late(mask).start()
        late_in[my_lane] = late_out[sp]

    @pl.when(is_owner)
    def _():
        query = jnp.sum(qslots[...], axis=0)
        mine_q = jnp.sum(jnp.where(row_head == my_head, query, 0.0), axis=0, keepdims=True)
        q_wide[...] = jnp.transpose(jnp.broadcast_to(mine_q, (LANES, DK)))

    def landed(line, part):
        settle(zrecv.at[line, part], z_send, z_recv.at[line, part]).wait_recv()
        return zrecv[line, part]

    def landed_gamma(line):
        settle(gzrecv.at[line], gz_send, gz_recv.at[line]).wait_recv()
        return gzrecv[line, 0:1, 0:1]

    def follow(line, state):
        gamma = landed_gamma(line)
        moved = gamma * state + mm(landed(line, 1), state)
        return moved + landed(line, 0).astype(F32) if line < 3 else moved

    for g in range(1, 1 + width_z):

        @pl.when(line_z == g)
        def _(g=g):
            own = maps[own_at]
            own_g = gams[own_at, 0:1, 0:1]
            if g == 1:
                gamma = landed_gamma(2)
                erase = landed(2, 1).astype(F32)
                both = gamma * own + mm(erase, own)
                both_b = both[:, :DV] + landed(2, 0).astype(F32)
                both_n = both[:, DV:] + own_g * erase
                first = landed(0, 0).astype(F32)
                state = (gamma * own_g) * first + mm(both_n, first) + both_b
            else:
                state = follow(1, landed(0, 0).astype(F32))
                state = own_g * state + mm(own[:, DV:], state) + own[:, :DV]
            final_ref[...] = follow(3, state)

    @pl.when(is_owner)
    def _():
        final = final_ref[...]
        raw_read = jnp.sum(final * q_wide[...], axis=0, keepdims=True)
        for j in range(n_sp):
            fstate[j, 0:rows_out, :] = final[j * rows_out : (j + 1) * rows_out, :]
            fstate[j, space : space + 1, :] = raw_read
        for mask in masks:
            copy_state(mask, my_head).start()
        srecv[my_head] = fstate[sp]

    settle(xg.at[pl.ds(0, 2 * n_y - 1)], tok_send, own_recv.at[0]).wait_send()
    settle(sendbuf, map_send, map_recv.at[0, 0]).wait_send()
    settle(gsend, g_send, g_recv.at[0]).wait_send()

    def depending(test, act, no, yes):
        for value, number in ((False, no), (True, yes)):

            @pl.when(test == value)
            def _(number=number):
                if number:
                    act(number)

    def queries_out(number):
        settle(qslots.at[pl.ds(0, number)], q_send, q_recv.at[0]).wait_send()

    depending(reads_query, queries_out, len(readers), len(readers) - 1)

    @pl.when(line_z == 0)
    def _():
        settle(zsend.at[:, 0], z_send, z_recv.at[0, 0]).wait_send()

    @pl.when(is_last)
    def _():
        settle(zsend.at[:, 1], z_send, z_recv.at[0, 0]).wait_send()
        settle(gzsend, gz_send, gz_recv.at[0]).wait_send()
        settle(late_out.at[pl.ds(0, len(masks))], l_send, l_recv.at[0]).wait_send()

    for line in range(1, 3):
        number = width_z - 1 if line <= width_z else width_z
        if number:

            @pl.when(line_z == line)
            def _(number=number):
                settle(zsend.at[pl.ds(0, number)], z_send, z_recv.at[0, 0]).wait_send()
                settle(gzsend.at[pl.ds(0, number)], gz_send, gz_recv.at[0]).wait_send()

    def late_ones(number):
        settle(late_in.at[pl.ds(0, number)], l_send, l_recv.at[0]).wait_recv()

    def states_in(number):
        settle(srecv.at[pl.ds(0, number)], s_send, s_recv.at[0]).wait_recv()

    depending(is_last, late_ones, lanes_of, lanes_of - 1)
    gain = gain_ref[...].astype(F32)
    depending(is_owner, states_in, heads, heads - 1)
    for h in range(heads):
        lane, i = h // width_z, h % width_z
        state_out[h] = (
            srecv[h, 0:rows_out, :] + late_in[lane, i * space : i * space + rows_out, :]
        ).astype(BF16)
        at = width_z * space + i
        raw = srecv[h, space : space + 1, :] + late_in[lane, at : at + 1, :]
        read_out[h : h + 1, :] = (
            raw * lax.rsqrt(jnp.mean(raw * raw, axis=-1, keepdims=True) + norm_eps) * gain
        )

    @pl.when(is_owner)
    def _():
        settle(fstate.at[pl.ds(0, len(masks))], s_send, s_recv.at[0]).wait_send()


def hand_over(state_ref, read_ref, state_out, read_out):
    state_out[...] = state_ref[...]
    read_out[...] = read_ref[...]


def per_device(
    n_sp,
    n_tp,
    tokens,
    w_key,
    w_value,
    w_beta,
    w_decay,
    beta_bias,
    decay_rate,
    forgetting_increment,
    new_query,
    read_gain,
):
    tokens_here, features = tokens.shape
    depth, width = w_key.shape
    heads = width // DK
    parts = tokens_here // CHUNK - 1 + tail_pieces(features)
    rows_out = DK // n_sp
    n_y = n_tp // 2
    total_heads = w_beta.shape[1]
    joins, splits, width_z, copies = tree_shape(n_sp, heads)
    space = -(-rows_out // SUB) * SUB
    slots = 0
    count = heads
    for _ in range(joins):
        count = max(count // 2, 1)
        slots += count
    vmem = pl.BlockSpec(memory_space=pltpu.VMEM)
    hbm = pl.BlockSpec(memory_space=pl.ANY)
    dma = pltpu.SemaphoreType.DMA
    state, read = pl.pallas_call(
        functools.partial(body, n_sp, n_tp),
        name="delta_state",
        out_shape=(
            pltpu.VMEM((heads, rows_out, DV), BF16),
            pltpu.VMEM((heads, DV), F32),
        ),
        in_specs=[hbm] * 10,
        out_specs=(vmem, vmem),
        scratch_shapes=[
            pltpu.VMEM((depth, width), BF16),
            pltpu.VMEM((depth, width), BF16),
            pltpu.VMEM(w_beta.shape[::-1], BF16),
            pltpu.VMEM(w_decay.shape[::-1], BF16),
            pltpu.VMEM((1, total_heads), F32),
            pltpu.VMEM((1, total_heads), F32),
            pltpu.VMEM(forgetting_increment.shape, F32),
            pltpu.VMEM(new_query.shape, BF16),
            pltpu.VMEM((1, DV), BF16),
            pltpu.VMEM((depth, LANES), BF16),
            pltpu.VMEM((tokens_here, features), BF16),
            pltpu.VMEM((SUB, tokens_here), F32),
            pltpu.VMEM((SUB, DK), F32),
            pltpu.VMEM((n_tp, tokens_here, features), BF16),
            pltpu.VMEM((tokens_here, width), F32),
            pltpu.VMEM((tokens_here, width), F32),
            pltpu.VMEM((tokens_here, LANES), F32),
            pltpu.VMEM((heads, DK, DV + DK), F32),
            pltpu.VMEM((heads, SUB, LANES), F32),
            pltpu.VMEM((slots, 2, DK, DV), BF16),
            pltpu.VMEM((slots, 2, DK, DV), BF16),
            pltpu.VMEM((slots, SUB, LANES), F32),
            pltpu.VMEM((slots, SUB, LANES), F32),
            pltpu.VMEM((width_z, 2, DK, DV), BF16),
            pltpu.VMEM((4, 2, DK, DV), BF16),
            pltpu.VMEM((width_z, SUB, LANES), F32),
            pltpu.VMEM((4, SUB, LANES), F32),
            pltpu.VMEM((n_sp, SUB, DK), F32),
            pltpu.VMEM((DK, LANES), F32),
            pltpu.VMEM((n_sp, space + SUB, DV), F32),
            pltpu.VMEM((DK, DV), F32),
            pltpu.VMEM((heads, space + SUB, DV), F32),
            pltpu.VMEM((n_sp, width_z * space + SUB, DV), F32),
            pltpu.VMEM((1 << splits, width_z * space + SUB, DV), F32),
            dma((10,)),
            pltpu.SemaphoreType.REGULAR((max(near_rounds(n_sp), 1),)),
            dma((1,)),
            dma((2 * (n_y - 1), parts)),
            dma((1,)),
            dma((slots, 2)),
            dma((joins,)),
            dma((4, 2)),
            dma((4,)),
            dma((1,)),
            dma((1,)),
        ],
        compiler_params=pltpu.CompilerParams(
            collective_id=0, has_side_effects=True, vmem_limit_bytes=63 * 1024 * 1024
        ),
    )(
        tokens,
        w_key,
        w_value,
        w_beta.T,
        w_decay.T,
        beta_bias[None, :],
        decay_rate[None, :],
        forgetting_increment,
        new_query,
        read_gain[None, :],
    )
    return pl.pallas_call(
        hand_over,
        name="hand_over",
        out_shape=(
            jax.ShapeDtypeStruct(state.shape, state.dtype),
            jax.ShapeDtypeStruct(read.shape, read.dtype),
        ),
        in_specs=[vmem, vmem],
        out_specs=(vmem, vmem),
    )(
        pltpu.with_memory_space_constraint(state, pltpu.VMEM),
        pltpu.with_memory_space_constraint(read, pltpu.VMEM),
    )


def solution(mesh):
    return jax.shard_map(
        functools.partial(per_device, mesh.shape["sp"], mesh.shape["tp"]),
        mesh=mesh,
        in_specs=(
            P("sp", "tp"),
            P(None, "tp"),
            P(None, "tp"),
            P(),
            P(),
            P(),
            P(),
            P("tp", "sp"),
            P("tp", "sp"),
            P(),
        ),
        out_specs=(P("tp", "sp", None), P("tp", None)),
        check_vma=False,
    )
```

```python
import functools

import jax
import jax.numpy as jnp
from jax import lax
from jax.experimental import pallas as pl
from jax.experimental.pallas import tpu as pltpu
from jax.sharding import PartitionSpec as P

DK = 128
DV = 128
CHUNK = 128
LANES = 128
SUB = 8
TILE = 16
norm_eps = 1e-06
MESH = pl.DeviceIdType.MESH
F32 = jnp.float32
BF16 = jnp.bfloat16


def mm(left, right):
    return jnp.dot(left.astype(BF16), right.astype(BF16), preferred_element_type=F32)


def mm_nt(left, right):
    return lax.dot_general(
        left.astype(BF16), right.astype(BF16), (((1,), (1,)), ((), ())), preferred_element_type=F32
    )


def log2(value):
    return value.bit_length() - 1


def near_rounds(n_sp):
    return 3 if n_sp == 8 else 0


def tree_shape(n_sp, heads):
    joins = log2(n_sp) - 2
    splits = min(joins, log2(heads))
    width_z = heads >> splits
    return joins, splits, width_z, 1 << (joins - splits)


def tail_pieces(features):
    return 4 if features % 1024 == 0 else 1


def body(
    n_sp,
    n_tp,
    x_hbm,
    wk_hbm,
    wv_hbm,
    wb_hbm,
    wd_hbm,
    bias_hbm,
    rate_hbm,
    finc_hbm,
    q_hbm,
    gain_hbm,
    state_out,
    read_out,
    wk,
    wv,
    wb,
    wd,
    bias_ref,
    rate_ref,
    finc_ref,
    q_ref,
    gain_ref,
    wg,
    x_ref,
    finc8,
    q_own,
    xg,
    acck,
    accv,
    accg,
    maps,
    gams,
    pair,
    sendbuf,
    recvbuf,
    gsend,
    grecv,
    zsend,
    zrecv,
    gzsend,
    gzrecv,
    qslots,
    q_wide,
    fstate,
    final_ref,
    srecv,
    late_out,
    late_in,
    wsem,
    ready,
    own_recv,
    tok_recv,
    q_recv,
    map_recv,
    g_recv,
    z_recv,
    gz_recv,
    s_recv,
    l_recv,
):
    sp = lax.axis_index("sp")
    tp = lax.axis_index("tp")
    tokens_here, features = x_ref.shape
    heads = wk.shape[1] // DK
    chunks = tokens_here // CHUNK
    last = chunks - 1
    pieces = tail_pieces(features)
    wide = features // pieces
    parts = last + pieces
    n_y = n_tp // 2
    y = tp // 2
    core = tp % 2
    sibling = tp + 1 - 2 * core
    levels = log2(n_sp)
    rows_out = DK // n_sp
    joins, splits, width_z, copies = tree_shape(n_sp, heads)
    base = 1 << joins
    line_z = sp // base

    (map_send, z_send, s_send, l_send, tok_send, q_send, g_send, gz_send) = (
        wsem.at[pl.ds(place, 1)] for place in range(8)
    )
    barrier = pltpu.get_barrier_semaphore()

    def tell(semaphore, place):
        pl.semaphore_signal(semaphore, inc=1, device_id=place, device_id_type=MESH)

    def flip(mask):
        found = sp
        for place in range(levels):
            if (mask >> place) % 2:
                found = found + (1 - 2 * ((sp // (1 << place)) % 2)) * (1 << place)
        return found

    line = sp // 2
    lines = n_sp // 2

    def tell_near(semaphore):
        tell(semaphore, {"sp": flip(1)})

        @pl.when(line > 0)
        def _():
            tell(semaphore, {"sp": sp - 2})

        @pl.when(line < lines - 1)
        def _():
            tell(semaphore, {"sp": sp + 2})

    near_count = 1 + jnp.where(line > 0, 1, 0) + jnp.where(line < lines - 1, 1, 0)
    rounds = near_rounds(n_sp)

    for step in range(1, n_y):
        peer = ((y + step) % n_y) * 2 + core
        tell(barrier, {"tp": peer})
    tell(barrier, {"tp": sibling})
    if rounds:
        tell_near(barrier)
        greeted = n_y + near_count
    else:
        for mask in range(1, n_sp):
            tell(barrier, {"sp": flip(mask)})
        greeted = n_y + n_sp - 1

    load_x = pltpu.make_async_copy(x_hbm, x_ref, wsem.at[4])
    load_x.start()
    small = [
        pltpu.make_async_copy(source, target, wsem.at[5 + place])
        for place, (source, target) in enumerate(
            (
                (q_hbm, q_ref),
                (finc_hbm, finc_ref),
                (bias_hbm, bias_ref),
                (rate_hbm, rate_ref),
                (gain_hbm, gain_ref),
            )
        )
    ]
    loads = [
        pltpu.make_async_copy(wk_hbm, wk, wsem.at[0]),
        pltpu.make_async_copy(wv_hbm, wv, wsem.at[1]),
        pltpu.make_async_copy(wb_hbm, wb, wsem.at[2]),
        pltpu.make_async_copy(wd_hbm, wd, wsem.at[3]),
    ]
    for load in (*small, loads[2], loads[3], loads[0], loads[1]):
        load.start()

    def part_of(k):
        if isinstance(k, int) and k >= last:
            return pl.ds(last * CHUNK, CHUNK), pl.ds((k - last) * wide, wide)
        start = k * CHUNK if isinstance(k, int) else pl.multiple_of(k * CHUNK, CHUNK)
        return pl.ds(start, CHUNK), pl.ds(0, features)

    def copy_own(source):
        return pltpu.make_async_remote_copy(
            src_ref=x_ref,
            dst_ref=xg.at[source],
            send_sem=tok_send.at[0],
            recv_sem=own_recv.at[0],
            device_id={"tp": sibling},
            device_id_type=MESH,
        )

    def copy_peer(step, k):
        rows, cols = part_of(k)
        peer = ((y + step) % n_y) * 2 + core
        return pltpu.make_async_remote_copy(
            src_ref=x_ref.at[rows, cols],
            dst_ref=xg.at[tp, rows, cols],
            send_sem=tok_send.at[0],
            recv_sem=tok_recv.at[step - 1, k],
            device_id={"tp": peer},
            device_id_type=MESH,
        )

    def copy_forward(step, k):
        rows, cols = part_of(k)
        source = ((y + n_y - step) % n_y) * 2 + core
        return pltpu.make_async_remote_copy(
            src_ref=xg.at[source, rows, cols],
            dst_ref=xg.at[source, rows, cols],
            send_sem=tok_send.at[0],
            recv_sem=tok_recv.at[n_y - 2 + step, k],
            device_id={"tp": sibling},
            device_id_type=MESH,
        )

    def arrived(source, place, k):
        rows, cols = part_of(k)
        pltpu.make_async_remote_copy(
            src_ref=xg.at[source, rows, cols],
            dst_ref=xg.at[source, rows, cols],
            send_sem=tok_send.at[0],
            recv_sem=tok_recv.at[place, k],
            device_id={"tp": sibling},
            device_id_type=MESH,
        ).wait_recv()

    pl.semaphore_wait(barrier, greeted)
    load_x.wait()
    for k in range(parts):
        for step in range(1, n_y):
            copy_peer(step, k).start()
        if k == 0:
            copy_own(tp).start()
    if rounds:
        tell_near(ready.at[0])
    for load in small:
        load.wait()

    rows_q = lax.broadcasted_iota(jnp.int32, (rows_out, LANES), 0)
    lanes_q = lax.broadcasted_iota(jnp.int32, (rows_out, LANES), 1)
    place_q = jnp.where(lanes_q == rows_q + sp * rows_out, 1.0, 0.0)
    q_own[...] = jnp.zeros_like(q_own)
    q_own[0:heads, :] = mm(q_ref[...], place_q)

    lead = heads // 2
    bit0 = sp % 2
    turn = jnp.where(line_z < 2, 1, 0)

    def actual(i):
        if heads == 1:
            return i
        found = (i + (1 - bit0) * lead) % heads
        return found + turn * (1 - 2 * (found % 2)) if lead == 2 else found

    finc8[...] = jnp.zeros_like(finc8)
    for i in range(heads):
        finc8[i : i + 1, :] = finc_ref[pl.ds(actual(i), 1), :]

    total_heads = wb.shape[0]
    row_id = lax.broadcasted_iota(jnp.int32, (LANES, total_heads), 0)
    col_id = lax.broadcasted_iota(jnp.int32, (LANES, total_heads), 1)
    first_head = tp * heads
    own_head = first_head + actual(row_id % SUB)
    own = (row_id % SUB < heads) & (col_id == own_head)
    pick_b = jnp.where(own & (row_id < SUB), 1.0, 0.0)
    pick_d = jnp.where(own & (row_id >= SUB) & (row_id < 2 * SUB), 1.0, 0.0)
    loads[2].wait()
    loads[3].wait()
    depth = wg.shape[0]
    piece = 512

    def pick(step, carry):
        rows = pl.ds(pl.multiple_of(step * piece, piece), piece)
        both = mm(pick_b, wb[:, rows]) + mm(pick_d, wd[:, rows])
        wg[rows, :] = jnp.transpose(both).astype(BF16)
        return carry

    lax.fori_loop(0, depth // piece, pick, 0)
    loads[0].wait()
    loads[1].wait()

    def project(x, source, rows, first=False, start=0, size=features):
        deep = pl.ds(pl.multiple_of(source * features + start, size), size)
        for acc, weights in ((acck, wk), (accv, wv), (accg, wg)):
            part = jnp.dot(x, weights[deep, :], preferred_element_type=F32)
            acc[rows, :] = part if first else acc[rows, :] + part

    half_rows = 256 if tokens_here % 256 == 0 else CHUNK

    def own_project(step, carry):
        rows = pl.ds(pl.multiple_of(step * half_rows, half_rows), half_rows)
        project(x_ref[rows, :], tp, rows, True)
        return carry

    lax.fori_loop(0, tokens_here // half_rows, own_project, 0)
    copy_own(sibling).wait_recv()
    for step in range(1, rounds):
        pl.semaphore_wait(ready.at[step - 1], near_count)
        tell_near(ready.at[step])

    def sibling_project(step, carry):
        rows = pl.ds(pl.multiple_of(step * half_rows, half_rows), half_rows)
        project(xg[sibling, rows, :], sibling, rows)
        return carry

    lax.fori_loop(0, tokens_here // half_rows, sibling_project, 0)
    if rounds:
        pl.semaphore_wait(ready.at[rounds - 1], near_count)

    lanes_of = 1 << splits

    def reader_of(h, copy):
        if h < heads:
            return (1 + h % width_z) * base + h // width_z + (copy << splits)
        return 3 * base + h - heads + (copy << splits)

    def copy_query(h, copy):
        owner = reader_of(h, copy)
        return pltpu.make_async_remote_copy(
            src_ref=q_own,
            dst_ref=qslots.at[sp],
            send_sem=q_send.at[0],
            recv_sem=q_recv.at[0],
            device_id={"sp": owner},
            device_id_type=MESH,
        )

    readers = [(h, copy) for h in range(heads + lanes_of) for copy in range(copies)]
    for h, copy in readers:

        @pl.when(sp != reader_of(h, copy))
        def _(h=h, copy=copy):
            copy_query(h, copy).start()

    row8 = lax.broadcasted_iota(jnp.int32, (SUB, total_heads), 0)
    lane8 = lax.broadcasted_iota(jnp.int32, (SUB, total_heads), 1)
    mine = (lane8 == first_head + actual(row8)) & (row8 < heads)
    bias_col = jnp.sum(jnp.where(mine, bias_ref[...], 0.0), axis=1, keepdims=True)
    rate_col = jnp.sum(jnp.where(mine, rate_ref[...], 0.0), axis=1, keepdims=True)

    maps[...] = jnp.zeros_like(maps)
    gams[...] = jnp.ones_like(gams)

    def near(step):
        return ((y + n_y - step) % n_y) * 2 + core

    def far(step):
        return ((y + n_y - step) % n_y) * 2 + 1 - core

    def gate_terms(rows):
        ri = lax.broadcasted_iota(jnp.int32, (CHUNK, CHUNK), 0)
        ci = lax.broadcasted_iota(jnp.int32, (CHUNK, CHUNK), 1)
        strict = ri > ci
        upper = jnp.where(ri <= ci, 1.0, 0.0).astype(BF16)
        gates = jnp.transpose(accg[rows, :])
        beta = jax.nn.sigmoid(gates[0:SUB, :] + bias_col)
        raw = gates[SUB : 2 * SUB, :]
        softplus = jnp.maximum(raw, 0.0) + jnp.log1p(jnp.exp(-jnp.abs(raw)))
        logd = -rate_col * softplus + finc8[:, rows]
        high = logd.astype(BF16).astype(F32)
        rest = logd - high
        middle = rest.astype(BF16).astype(F32)
        thirds = jnp.concatenate([high, middle, rest - middle], axis=0)
        sums = mm(thirds, upper)
        cum = sums[0:SUB] + sums[SUB : 2 * SUB] + sums[2 * SUB :]
        total = jnp.sum(logd, axis=1, keepdims=True)
        columns = jnp.transpose(
            jnp.concatenate(
                [
                    beta,
                    cum,
                    jnp.exp(cum),
                    jnp.exp(total - cum),
                    jnp.zeros((LANES - 4 * SUB, LANES), F32),
                ],
                axis=0,
            )
        )
        return strict, cum, columns, jnp.exp(total)

    def prepare(rows, chosen):
        found = []
        for h in chosen:
            cols = pl.ds(pl.multiple_of(actual(h) * DK, DK), DK)
            key = acck[rows, cols].astype(BF16).astype(F32)
            key = key * lax.rsqrt(jnp.sum(key * key, axis=-1, keepdims=True) + norm_eps)
            seen = mm(key, maps[h])
            erased = jnp.concatenate([seen[:, :DV], seen[:, DV:] + gams[h, 0:1, 0:1] * key], axis=1)
            found.append((key, mm_nt(key, key), erased))
        return found

    def advance(rows, terms, chosen, found=None, pause=None):
        strict, cum, columns, keep = terms
        found = prepare(rows, chosen) if found is None else found
        solved, powers, remains = [], [], []
        for h, (key, pairs, erased) in zip(chosen, found):
            cols = pl.ds(pl.multiple_of(actual(h) * DK, DK), DK)
            value = accv[rows, cols].astype(BF16).astype(F32)
            b_col = columns[:, h : h + 1]
            c_col = columns[:, SUB + h : SUB + h + 1]
            e_col = columns[:, 2 * SUB + h : 2 * SUB + h + 1]
            r_col = columns[:, 3 * SUB + h : 3 * SUB + h + 1]
            decay = jnp.exp(jnp.where(strict, c_col - cum[h : h + 1, :], 0.0))
            powers.append(jnp.where(strict, pairs * (b_col * decay), 0.0))
            gone = (b_col * e_col) * erased
            solved.append(jnp.concatenate([value * b_col - gone[:, :DV], -gone[:, DV:]], axis=1))
            remains.append(jnp.transpose(key * r_col))
        solved = [right - mm(power, right) for power, right in zip(powers, solved)]
        covered = 2
        while covered < CHUNK:
            powers = [mm(power, power) for power in powers]
            solved = [known + mm(power, known) for power, known in zip(powers, solved)]
            covered *= 2
            if covered == 16 and pause is not None:
                pause()
        for h, remain, new in zip(chosen, remains, solved):
            maps[h] = keep[h : h + 1, 0:1] * maps[h] + mm(remain, new)
            gams[h] = keep[h : h + 1, 0:1] * gams[h]

    def near_take(k):
        for step in range(1, n_y):
            arrived(near(step), step - 1, k)
            copy_forward(step, k).start()

    def far_take(k):
        for step in range(1, n_y):
            arrived(far(step), n_y - 2 + step, k)

    def take_in(side, rows):
        for step in range(1, n_y):
            project(xg[side(step), rows, :], side(step), rows)

    def chunk_step(c, carry):
        rows = pl.ds(pl.multiple_of(c * CHUNK, CHUNK), CHUNK)
        near_take(c)
        take_in(near, rows)
        far_take(c)
        take_in(far, rows)
        advance(rows, gate_terms(rows), range(heads))
        return carry

    end_rows = pl.ds(last * CHUNK, CHUNK)

    def end_project(side, place, number):
        cols = pl.ds(place * wide, number * wide)
        for step in range(1, n_y):
            project(
                xg[side(step), end_rows, cols],
                side(step),
                end_rows,
                False,
                place * wide,
                number * wide,
            )

    if pieces == 4 and last > 1:
        lax.fori_loop(0, last - 1, chunk_step, 0)
        before = last - 1
        rows = pl.ds(before * CHUNK, CHUNK)
        near_take(before)
        take_in(near, rows)

        @pl.when(core == 1)
        def _():
            near_take(last)
            near_take(last + 1)

        far_take(before)
        take_in(far, rows)

        @pl.when(core == 1)
        def _():
            near_take(last + 2)

        def pause():
            @pl.when(core == 1)
            def _():
                near_take(last + 3)

        advance(rows, gate_terms(rows), range(heads), pause=pause)

        @pl.when(core == 1)
        def _():
            end_project(near, 0, 4)
            far_take(last)
            far_take(last + 1)
            end_project(far, 0, 2)
            far_take(last + 2)
            far_take(last + 3)
            end_project(far, 2, 2)

        @pl.when(core == 0)
        def _():
            near_take(last)
            near_take(last + 1)
            end_project(near, 0, 2)
            near_take(last + 2)
            far_take(last)
            far_take(last + 1)
            end_project(far, 0, 2)
            end_project(near, 2, 1)
            far_take(last + 2)
            near_take(last + 3)
            far_take(last + 3)
            end_project(far, 2, 2)
            end_project(near, 3, 1)
    else:
        lax.fori_loop(0, last, chunk_step, 0)
        for place in range(pieces):
            near_take(last + place)
            end_project(near, place, 1)
        for place in range(pieces):
            far_take(last + place)
            end_project(far, place, 1)
    first_out = range(heads // 2 if heads > 1 else heads)
    end_found = prepare(end_rows, first_out)
    end_terms = gate_terms(end_rows)

    def copy_map(slot, part, partner):
        return pltpu.make_async_remote_copy(
            src_ref=sendbuf.at[slot, part],
            dst_ref=recvbuf.at[slot, part],
            send_sem=map_send.at[0],
            recv_sem=map_recv.at[slot, part],
            device_id={"sp": partner},
            device_id_type=MESH,
        )

    def copy_gamma(level, slot, number, partner):
        slots = pl.ds(slot, number)
        return pltpu.make_async_remote_copy(
            src_ref=gsend.at[slots],
            dst_ref=grecv.at[slots],
            send_sem=g_send.at[0],
            recv_sem=g_recv.at[level],
            device_id={"sp": partner},
            device_id_type=MESH,
        )

    def goal(j):
        return 1 + (turn + j) % 2 if width_z == 2 else 1

    def copy_up(j, part):
        return pltpu.make_async_remote_copy(
            src_ref=zsend.at[j, part],
            dst_ref=zrecv.at[line_z, part],
            send_sem=z_send.at[0],
            recv_sem=z_recv.at[line_z, part],
            device_id={"sp": sp % base + goal(j) * base},
            device_id_type=MESH,
        )

    def copy_up_gamma(j):
        return pltpu.make_async_remote_copy(
            src_ref=gzsend.at[j],
            dst_ref=gzrecv.at[line_z],
            send_sem=gz_send.at[0],
            recv_sem=gz_recv.at[line_z],
            device_id={"sp": sp % base + goal(j) * base},
            device_id_type=MESH,
        )

    count = heads
    offset = 0
    held = 0
    for level in range(joins):
        bit = (sp // (1 << level)) % 2
        later = bit == 1
        partner = flip(1 << level)
        split = count > 1
        half = count // 2 if split else count
        if level == 0:
            send_at, keep_at = 0, heads - half
        else:
            keep_at = held + (bit * half if split else 0)
            send_at = held + ((1 - bit) * half if split else 0)
        for j in range(half):
            if level == 0:
                gsend[j] = end_terms[3][j : j + 1, 0:1] * gams[j]
            else:
                gsend[offset + j] = gams[send_at + j]
        copy_gamma(level, offset, half, partner).start()
        if level == 0:
            advance(end_rows, end_terms, first_out, end_found)
        top = level == joins - 1
        for j in range(half):
            for part in (1, 0):
                cols = pl.ds(part * DV, DV)
                sendbuf[offset + j, part] = maps[send_at + j, :, cols].astype(BF16)
        usual = [(j, part) for j in range(half) for part in (1, 0)]
        erase_first = [(j, part) for part in (1, 0) for j in range(half)]

        def start_all(order):
            for j, part in order:
                copy_map(offset + j, part, partner).start()

        if top and half > 1:

            @pl.when(line_z < 3)
            def _():
                start_all(usual)

            @pl.when(line_z == 3)
            def _():
                start_all(erase_first)

        else:
            start_all(usual)
        if level == 0 and split:
            advance(end_rows, end_terms, range(half, heads))
        copy_gamma(level, offset, half, partner).wait_recv()
        if top:
            for j in range(half):
                gzsend[j] = gams[keep_at + j] * grecv[offset + j]

                @pl.when(jnp.logical_and(line_z != goal(j), line_z > 0))
                def _(j=j):
                    copy_up_gamma(j).start()

        def sides(j, part):
            own = maps[keep_at + j, :, pl.ds(part * DV, DV)]
            if not split:
                own = own.astype(BF16).astype(F32)
            got = recvbuf[offset + j, part].astype(F32)
            return jnp.where(later, own, got), jnp.where(later, got, own)

        def join(j, part):
            own_g, got_g = gams[keep_at + j], grecv[offset + j]
            copy_map(offset + j, part, partner).wait_recv()
            left_g = jnp.where(later, own_g, got_g)[0:1, 0:1]
            right_g = jnp.where(later, got_g, own_g)[0:1, 0:1]
            left, right = sides(j, part)
            if part:
                return left_g * right + mm(left, right) + right_g * left
            return left_g * right + mm(sides(j, 1)[0], right) + left

        def join_top(j, part):
            joined = join(j, part)
            pair[j, :, pl.ds(part * DV, DV)] = joined
            zsend[j, part] = joined.astype(BF16)
            sends = line_z > 0 if part else line_z < 3

            @pl.when(jnp.logical_and(line_z != goal(j), sends))
            def _():
                copy_up(j, part).start()

        if not top:
            for j in range(half):
                both = [join(j, part) for part in (0, 1)]
                maps[keep_at + j] = jnp.concatenate(both, axis=1)
                gams[keep_at + j] = gams[keep_at + j] * grecv[offset + j]
        elif half == 2:
            join_top(0, 1)

            @pl.when(line_z < 3)
            def _():
                join_top(0, 0)

            join_top(1, 1)

            @pl.when(line_z == 3)
            def _():
                join_top(0, 0)

            join_top(1, 0)
        else:
            for j, part in usual:
                join_top(j, part)
        offset += half
        count = half
        held = keep_at

    def copy_state(mask, h):
        target = flip(mask)
        return pltpu.make_async_remote_copy(
            src_ref=fstate.at[target],
            dst_ref=srecv.at[h],
            send_sem=s_send.at[0],
            recv_sem=s_recv.at[0],
            device_id={"sp": target},
            device_id_type=MESH,
        )

    def copy_late(mask):
        target = flip(mask)
        return pltpu.make_async_remote_copy(
            src_ref=late_out.at[target],
            dst_ref=late_in.at[sp % lanes_of],
            send_sem=l_send.at[0],
            recv_sem=l_recv.at[0],
            device_id={"sp": target},
            device_id_type=MESH,
        )

    def settle(ref, sent, landed):
        return pltpu.make_async_remote_copy(
            src_ref=ref,
            dst_ref=ref,
            send_sem=sent.at[0],
            recv_sem=landed,
            device_id={"sp": sp},
            device_id_type=MESH,
        )

    free = [1 << place for place in range(levels) if place < splits or place >= joins]
    masks = [0]
    for place in reversed(free):
        masks = [mask + more for more in (place, 0) for mask in masks]
    masks = [mask for mask in sorted(masks, key=lambda mask: (mask // base % 4 != 2, -(mask % base))) if mask]
    is_owner = jnp.logical_and(line_z >= 1, line_z <= width_z)
    is_last = line_z == 3
    reads_query = jnp.logical_or(is_owner, is_last)
    my_lane = sp % lanes_of
    my_head = my_lane * width_z + line_z - 1
    own_at = width_z - 1
    space = srecv.shape[1] - TILE

    def three_rows(row):
        high = row.astype(BF16)
        rest = row - high.astype(F32)
        middle = rest.astype(BF16)
        return high, middle, (rest - middle.astype(F32)).astype(BF16)

    def one_row(ref, lead_at, at):
        found = ref[lead_at, at : at + 8, :].astype(F32)
        return found[0:1] + found[1:2] + found[2:3]

    row_head = lax.broadcasted_iota(jnp.int32, (SUB, DK), 0)

    @pl.when(reads_query)
    def _():
        settle(qslots.at[pl.ds(0, n_sp - 1)], q_send, q_recv.at[0]).wait_recv()
        qslots[sp] = q_own[...]

    @pl.when(is_last)
    def _():
        query = jnp.sum(qslots[...], axis=0)
        for i in range(width_z):
            part = pair[i, :, :DV]
            reads = mm(query, part)
            wanted = row_head == my_lane * width_z + i
            line_read = jnp.sum(jnp.where(wanted, reads, 0.0), axis=0, keepdims=True)
            at = width_z * space + i * SUB
            rounded = part.astype(BF16)
            block = jnp.concatenate([*three_rows(line_read), jnp.zeros((SUB - 3, DV), BF16)], axis=0)
            for j in range(n_sp):
                late_out[j, i * space : i * space + rows_out, :] = rounded[
                    j * rows_out : (j + 1) * rows_out, :
                ]
                late_out[j, at : at + SUB, :] = block
        for mask in sorted(masks, reverse=True):
            copy_late(mask).start()
        late_in[my_lane] = late_out[sp]

    @pl.when(is_owner)
    def _():
        query = jnp.sum(qslots[...], axis=0)
        mine_q = jnp.sum(jnp.where(row_head == my_head, query, 0.0), axis=0, keepdims=True)
        q_wide[...] = jnp.transpose(jnp.broadcast_to(mine_q, (LANES, DK)))

    def landed(line, part):
        settle(zrecv.at[line, part], z_send, z_recv.at[line, part]).wait_recv()
        return zrecv[line, part]

    def landed_gamma(line):
        settle(gzrecv.at[line], gz_send, gz_recv.at[line]).wait_recv()
        return gzrecv[line, 0:1, 0:1]

    def follow(line, state):
        gamma = landed_gamma(line)
        moved = gamma * state + mm(landed(line, 1), state)
        return moved + landed(line, 0).astype(F32) if line < 3 else moved

    for g in range(1, 1 + width_z):

        @pl.when(line_z == g)
        def _(g=g):
            own = pair[own_at]
            own_g = gzsend[own_at, 0:1, 0:1]
            if g == 1:
                gamma = landed_gamma(2)
                erase = landed(2, 1).astype(F32)
                both = gamma * own + mm(erase, own)
                both_b = both[:, :DV] + landed(2, 0).astype(F32)
                both_n = both[:, DV:] + own_g * erase
                first = landed(0, 0).astype(F32)
                state = (gamma * own_g) * first + mm(both_n, first) + both_b
            else:
                state = follow(1, landed(0, 0).astype(F32))
                state = own_g * state + mm(own[:, DV:], state) + own[:, :DV]
            final_ref[...] = follow(3, state)

    @pl.when(is_owner)
    def _():
        final = final_ref[...]
        raw_read = jnp.sum(final * q_wide[...], axis=0, keepdims=True)
        rounded = final.astype(BF16)
        block = jnp.concatenate([*three_rows(raw_read), jnp.zeros((SUB - 3, DV), BF16)], axis=0)
        for j in range(n_sp):
            fstate[j, 0:rows_out, :] = rounded[j * rows_out : (j + 1) * rows_out, :]
            fstate[j, space : space + SUB, :] = block
        for mask in masks:
            copy_state(mask, my_head).start()
        srecv[my_head] = fstate[sp]

    settle(xg.at[pl.ds(0, 2 * n_y - 1)], tok_send, own_recv.at[0]).wait_send()
    settle(sendbuf, map_send, map_recv.at[0, 0]).wait_send()
    settle(gsend, g_send, g_recv.at[0]).wait_send()

    def depending(test, act, no, yes):
        for value, number in ((False, no), (True, yes)):

            @pl.when(test == value)
            def _(number=number):
                if number:
                    act(number)

    def queries_out(number):
        settle(qslots.at[pl.ds(0, number)], q_send, q_recv.at[0]).wait_send()

    depending(reads_query, queries_out, len(readers), len(readers) - 1)

    @pl.when(line_z == 0)
    def _():
        settle(zsend.at[:, 0], z_send, z_recv.at[0, 0]).wait_send()

    @pl.when(is_last)
    def _():
        settle(zsend.at[:, 1], z_send, z_recv.at[0, 0]).wait_send()
        settle(gzsend, gz_send, gz_recv.at[0]).wait_send()
        settle(late_out.at[pl.ds(0, len(masks))], l_send, l_recv.at[0]).wait_send()

    for line in range(1, 3):
        number = width_z - 1 if line <= width_z else width_z
        if number:

            @pl.when(line_z == line)
            def _(number=number):
                settle(zsend.at[pl.ds(0, number)], z_send, z_recv.at[0, 0]).wait_send()
                settle(gzsend.at[pl.ds(0, number)], gz_send, gz_recv.at[0]).wait_send()

    def late_ones(number):
        settle(late_in.at[pl.ds(0, number)], l_send, l_recv.at[0]).wait_recv()

    def states_in(number):
        settle(srecv.at[pl.ds(0, number)], s_send, s_recv.at[0]).wait_recv()

    depending(is_last, late_ones, lanes_of, lanes_of - 1)
    gain = gain_ref[...].astype(F32)
    depending(is_owner, states_in, heads, heads - 1)
    for h in range(heads):
        lane, i = h // width_z, h % width_z
        state_out[h] = (
            srecv[h, 0:rows_out, :].astype(F32)
            + late_in[lane, i * space : i * space + rows_out, :].astype(F32)
        ).astype(BF16)
        raw = one_row(srecv, h, space) + one_row(late_in, lane, width_z * space + i * SUB)
        read_out[h : h + 1, :] = (
            raw * lax.rsqrt(jnp.mean(raw * raw, axis=-1, keepdims=True) + norm_eps) * gain
        )

    @pl.when(is_owner)
    def _():
        settle(fstate.at[pl.ds(0, len(masks))], s_send, s_recv.at[0]).wait_send()


def hand_over(state_ref, read_ref, state_out, read_out):
    state_out[...] = state_ref[...]
    read_out[...] = read_ref[...]


def per_device(
    n_sp,
    n_tp,
    tokens,
    w_key,
    w_value,
    w_beta,
    w_decay,
    beta_bias,
    decay_rate,
    forgetting_increment,
    new_query,
    read_gain,
):
    tokens_here, features = tokens.shape
    depth, width = w_key.shape
    heads = width // DK
    parts = tokens_here // CHUNK - 1 + tail_pieces(features)
    rows_out = DK // n_sp
    n_y = n_tp // 2
    total_heads = w_beta.shape[1]
    joins, splits, width_z, copies = tree_shape(n_sp, heads)
    space = -(-rows_out // TILE) * TILE
    slots = 0
    count = heads
    for _ in range(joins):
        count = max(count // 2, 1)
        slots += count
    vmem = pl.BlockSpec(memory_space=pltpu.VMEM)
    hbm = pl.BlockSpec(memory_space=pl.ANY)
    dma = pltpu.SemaphoreType.DMA
    state, read = pl.pallas_call(
        functools.partial(body, n_sp, n_tp),
        name="delta_state",
        out_shape=(
            pltpu.VMEM((heads, rows_out, DV), BF16),
            pltpu.VMEM((heads, DV), F32),
        ),
        in_specs=[hbm] * 10,
        out_specs=(vmem, vmem),
        scratch_shapes=[
            pltpu.VMEM((depth, width), BF16),
            pltpu.VMEM((depth, width), BF16),
            pltpu.VMEM(w_beta.shape[::-1], BF16),
            pltpu.VMEM(w_decay.shape[::-1], BF16),
            pltpu.VMEM((1, total_heads), F32),
            pltpu.VMEM((1, total_heads), F32),
            pltpu.VMEM(forgetting_increment.shape, F32),
            pltpu.VMEM(new_query.shape, BF16),
            pltpu.VMEM((1, DV), BF16),
            pltpu.VMEM((depth, LANES), BF16),
            pltpu.VMEM((tokens_here, features), BF16),
            pltpu.VMEM((SUB, tokens_here), F32),
            pltpu.VMEM((SUB, DK), F32),
            pltpu.VMEM((n_tp, tokens_here, features), BF16),
            pltpu.VMEM((tokens_here, width), F32),
            pltpu.VMEM((tokens_here, width), F32),
            pltpu.VMEM((tokens_here, LANES), F32),
            pltpu.VMEM((heads, DK, DV + DK), F32),
            pltpu.VMEM((heads, SUB, LANES), F32),
            pltpu.VMEM((width_z, DK, DV + DK), F32),
            pltpu.VMEM((slots, 2, DK, DV), BF16),
            pltpu.VMEM((slots, 2, DK, DV), BF16),
            pltpu.VMEM((slots, SUB, LANES), F32),
            pltpu.VMEM((slots, SUB, LANES), F32),
            pltpu.VMEM((width_z, 2, DK, DV), BF16),
            pltpu.VMEM((4, 2, DK, DV), BF16),
            pltpu.VMEM((width_z, SUB, LANES), F32),
            pltpu.VMEM((4, SUB, LANES), F32),
            pltpu.VMEM((n_sp, SUB, DK), F32),
            pltpu.VMEM((DK, LANES), F32),
            pltpu.VMEM((n_sp, space + TILE, DV), BF16),
            pltpu.VMEM((DK, DV), F32),
            pltpu.VMEM((heads, space + TILE, DV), BF16),
            pltpu.VMEM((n_sp, width_z * space + TILE, DV), BF16),
            pltpu.VMEM((1 << splits, width_z * space + TILE, DV), BF16),
            dma((10,)),
            pltpu.SemaphoreType.REGULAR((max(near_rounds(n_sp), 1),)),
            dma((1,)),
            dma((2 * (n_y - 1), parts)),
            dma((1,)),
            dma((slots, 2)),
            dma((joins,)),
            dma((4, 2)),
            dma((4,)),
            dma((1,)),
            dma((1,)),
        ],
        compiler_params=pltpu.CompilerParams(
            collective_id=0, has_side_effects=True, vmem_limit_bytes=63 * 1024 * 1024
        ),
    )(
        tokens,
        w_key,
        w_value,
        w_beta.T,
        w_decay.T,
        beta_bias[None, :],
        decay_rate[None, :],
        forgetting_increment,
        new_query,
        read_gain[None, :],
    )
    return pl.pallas_call(
        hand_over,
        name="hand_over",
        out_shape=(
            jax.ShapeDtypeStruct(state.shape, state.dtype),
            jax.ShapeDtypeStruct(read.shape, read.dtype),
        ),
        in_specs=[vmem, vmem],
        out_specs=(vmem, vmem),
    )(
        pltpu.with_memory_space_constraint(state, pltpu.VMEM),
        pltpu.with_memory_space_constraint(read, pltpu.VMEM),
    )


def solution(mesh):
    return jax.shard_map(
        functools.partial(per_device, mesh.shape["sp"], mesh.shape["tp"]),
        mesh=mesh,
        in_specs=(
            P("sp", "tp"),
            P(None, "tp"),
            P(None, "tp"),
            P(),
            P(),
            P(),
            P(),
            P("tp", "sp"),
            P("tp", "sp"),
            P(),
        ),
        out_specs=(P("tp", "sp", None), P("tp", None)),
        check_vma=False,
    )
```
